768 devices in a mesh: sp: 192 (over z, y, core), tp: 4 (over x).
Axes of the slice: x: 4, y: 8, z: 12, core: 2. Of those that a mesh axis runs over, the one named last changes fastest.
Arguments:
- query_rows: bfloat16 [196608, 1024], P(('sp', 'tp')), may hold values from -6 to 6
- key_rows: bfloat16 [196608, 1024], P(('sp', 'tp')), may hold values from -6 to 6
- value_rows: bfloat16 [196608, 1024], P(('sp', 'tp')), may hold values from -6 to 6
- out_grad: bfloat16 [196608, 1024], P(('sp', 'tp')), may hold values from -40 to 40
- log_totals: float32 [196608, 8], P(('sp', 'tp')), may hold values from 6 to 7.5
- out_dot: float32 [196608, 8], P(('sp', 'tp')), may hold values from -6 to 6
- bias_table: float32 [8, 320], replicated, may hold values from -4 to 4
Outputs:
- grad_query: bfloat16 [196608, 1024], P(('sp', 'tp'))
- grad_key: bfloat16 [196608, 1024], P(('sp', 'tp'))
- grad_value: bfloat16 [196608, 1024], P(('sp', 'tp'))
- grad_table: float32 [8, 320], replicated
The draws below stay inside these ranges and needn't reach their ends.
All inputs are finite; a program needn't handle non-finite values.
Results may differ from the reference program's by a relative error of at most 0.005.
Values may be sent and summed in bfloat16 or wider, within the bound.
A program may use at most 128 MiB of HBM per device.

```python
import jax
import jax.numpy as jnp
from jax import lax

HEADS = 8
HEAD_DIM = 128
SEG_LEN = 64
LEFT_SEGS = 8
REL_CLIP = 256
TOK_DEV = 256
MIX_WIDTH = 1024
TABLE_LEN = 320
BACK_DEVS = 2
TOKENS = 196608


def draw_out_grad(key, part):
    position = jnp.arange(TOKENS, dtype=jnp.float32) / TOKENS
    base_vals = jnp.clip(jax.random.normal(key, (TOKENS, HEADS * HEAD_DIM), jnp.float32), -6.0, 6.0)
    growth = 3.0 ** position
    return (base_vals * growth[:, None]).astype(jnp.bfloat16)


def block_levels(rng, shape, shards, low, largest):
    loudness, own = 1.0, jax.random.fold_in(rng, 6)
    for axis_at, shards_of in shards:
        heights = jnp.exp(jax.random.uniform(jax.random.fold_in(own, axis_at), (shards_of,), jnp.float32, low / len(shards), largest / len(shards)))
        loudness = loudness * jnp.repeat(heights, shape[axis_at] // shards_of).reshape([-1 if axis == axis_at else 1 for axis in range(len(shape))])
    return loudness


def noise(key, shape, deviation, bound, cuts=(), held_as=jnp.bfloat16):
    entries = jax.random.normal(key, shape, jnp.float32) * deviation
    if len(cuts) > 0:
        entries = block_levels(key, shape, cuts, -0.22, 0.18) * entries
    return jnp.clip(entries, min=-bound, max=bound).astype(held_as)


def setup_inputs(seed: int = 0) -> dict:
    key_of = jax.random.split(jax.random.key(seed), 8)
    query_rows = noise(key_of[0], (TOKENS, MIX_WIDTH), 1.0, 6.0, ((0, 768),))
    key_rows = noise(key_of[1], (TOKENS, MIX_WIDTH), 1.0, 6.0, ((0, 768),))
    value_rows = noise(key_of[2], (TOKENS, MIX_WIDTH), 1.0, 6.0, ((0, 768),))
    out_grad = draw_out_grad(jax.random.fold_in(key_of[7], 71), 0)
    log_totals = jnp.clip(6.0 + 1.5 * jax.random.uniform(key_of[4], (TOKENS, HEADS), jnp.float32) ** block_levels(key_of[4], (TOKENS, HEADS), ((0, 768),), -0.2, 0.2), 6.0, 7.5)
    out_dot = noise(key_of[5], (TOKENS, HEADS), 1.5, 6.0, ((0, 768),), jnp.float32)
    bias_table = noise(key_of[6], (HEADS, TABLE_LEN), 1.0, 4.0, (), jnp.float32)
    return dict(query_rows=query_rows, key_rows=key_rows, value_rows=value_rows, out_grad=out_grad, log_totals=log_totals, out_dot=out_dot, bias_table=bias_table)


def reference(query_rows, key_rows, value_rows, out_grad, log_totals, out_dot, bias_table):
    token_count = query_rows.shape[0]
    feature_count = query_rows.shape[1]
    head_count = bias_table.shape[0]
    head_size = feature_count // head_count
    block_rows = TOK_DEV
    lag_rows = BACK_DEVS * TOK_DEV
    window = lag_rows + block_rows
    inv_root = head_size ** -0.5
    padded_keys = jnp.concatenate([jnp.zeros((lag_rows, feature_count), query_rows.dtype), key_rows], axis=0)
    padded_values = jnp.concatenate([jnp.zeros((lag_rows, feature_count), query_rows.dtype), value_rows], axis=0)
    local_query = jnp.arange(block_rows, dtype=jnp.int32)
    local_key = jnp.arange(window, dtype=jnp.int32)
    distance = local_query[:, None] - local_key[None, :] + lag_rows
    table_index = (jnp.clip(distance, 1 - SEG_LEN, REL_CLIP) + SEG_LEN - 1).astype(jnp.int32)
    bias_vals = bias_table[:, table_index]
    seg_gap = (local_query[:, None] + lag_rows) // SEG_LEN - (local_key // SEG_LEN)[None, :]
    band_ok = (seg_gap >= 0) & (seg_gap <= LEFT_SEGS)

    def one_block(totals, block_id):
        key_grads, value_grads, table_grad = totals
        first_row = (block_id * block_rows).astype(jnp.int32)
        queries = lax.dynamic_slice_in_dim(query_rows, first_row, block_rows, 0).astype(jnp.float32)
        queries = queries.reshape(block_rows, head_count, head_size)
        grads_out = lax.dynamic_slice_in_dim(out_grad, first_row, block_rows, 0).astype(jnp.float32)
        grads_out = grads_out.reshape(block_rows, head_count, head_size)
        log_rows = lax.dynamic_slice_in_dim(log_totals, first_row, block_rows, 0)
        dot_rows = lax.dynamic_slice_in_dim(out_dot, first_row, block_rows, 0)
        keys = lax.dynamic_slice_in_dim(padded_keys, first_row, window, 0).astype(jnp.float32)
        keys = keys.reshape(window, head_count, head_size)
        values = lax.dynamic_slice_in_dim(padded_values, first_row, window, 0).astype(jnp.float32)
        values = values.reshape(window, head_count, head_size)
        allowed = band_ok & ((first_row - lag_rows + local_key) >= 0)[None, :]
        scores = jnp.einsum('phd,rhd->hpr', queries, keys) * inv_root + bias_vals
        weights = jnp.where(allowed[None], jnp.exp(scores - log_rows.T[:, :, None]), 0.0)
        weights_b = lax.optimization_barrier(weights.astype(jnp.bfloat16)).astype(jnp.float32)
        weight_grads = jnp.einsum('phd,rhd->hpr', grads_out, values)
        score_grads = weights * (weight_grads - dot_rows.T[:, :, None])
        score_grads_b = lax.optimization_barrier(score_grads.astype(jnp.bfloat16)).astype(jnp.float32)
        block_query = jnp.einsum('hpr,rhd->phd', score_grads_b, keys) * inv_root
        block_key = (jnp.einsum('hpr,phd->rhd', score_grads_b, queries) * inv_root).reshape(window, feature_count)
        block_value = jnp.einsum('hpr,phd->rhd', weights_b, grads_out).reshape(window, feature_count)
        table_part = jax.ops.segment_sum(score_grads.reshape(head_count, -1).T, table_index.reshape(-1),
                                         num_segments=TABLE_LEN).T
        key_grads = lax.dynamic_update_slice_in_dim(
            key_grads, lax.dynamic_slice_in_dim(key_grads, first_row, window, 0) + block_key, first_row, 0)
        value_grads = lax.dynamic_update_slice_in_dim(
            value_grads, lax.dynamic_slice_in_dim(value_grads, first_row, window, 0) + block_value, first_row, 0)
        result_rows = block_query.reshape(block_rows, feature_count).astype(jnp.bfloat16)
        return (key_grads, value_grads, table_grad + table_part), result_rows

    start_totals = (jnp.zeros((lag_rows + token_count, feature_count), jnp.float32),
                    jnp.zeros((lag_rows + token_count, feature_count), jnp.float32),
                    jnp.zeros((head_count, TABLE_LEN), jnp.float32))
    block_ids = jnp.arange(token_count // block_rows, dtype=jnp.int32)
    (key_grads, value_grads, table_grad), query_grads = lax.scan(one_block, start_totals, block_ids)
    grad_query = query_grads.reshape(token_count, feature_count)
    grad_key = key_grads[lag_rows:].astype(jnp.bfloat16)
    grad_value = value_grads[lag_rows:].astype(jnp.bfloat16)
    return (grad_query, grad_key, grad_value, table_grad)
```

```python
import functools
import math

import jax
import jax.numpy as jnp
from jax import lax
from jax.experimental import pallas as pl
from jax.experimental.pallas import tpu as pltpu
from jax.sharding import PartitionSpec as P

SEG_LEN = 64
REL_CLIP = 256
ROWS = 256
HALF = 128
BAND = 640
HEADS = 8
HEAD_DIM = 128
TABLE_LEN = 320
LOG2E = math.log2(math.e)
FAR = 1e30
MESH = pl.DeviceIdType.MESH
F32 = jnp.float32
BF16 = jnp.bfloat16


def dot_nt(lhs, rhs):
    return lax.dot_general(lhs, rhs, (((1,), (1,)), ((), ())), preferred_element_type=F32)


def dot_nn(lhs, rhs):
    return lax.dot_general(lhs, rhs, (((1,), (0,)), ((), ())), preferred_element_type=F32)


def dot_tn(lhs, rhs):
    return lax.dot_general(lhs, rhs, (((0,), (0,)), ((), ())), preferred_element_type=F32)


def kernel(
    sp_size,
    tp_size,
    q_hbm,
    k_hbm,
    v_hbm,
    g_hbm,
    lse_hbm,
    dot_hbm,
    table_ref,
    dq_hbm,
    dk_hbm,
    dv_hbm,
    gt_ref,
    kv,
    qg,
    stats,
    wide,
    bias,
    ext,
    acc,
    outs,
    load_sem,
    stat_sem,
    out_sem,
    kv_send,
    kv_recv,
    qg_send,
    qg_recv,
    st_send,
    st_recv,
):
    sp, tp = lax.axis_index("sp"), lax.axis_index("tp")
    last_tp, first_tp = tp == tp_size - 1, tp == 0
    nxt = (
        lax.rem(sp + jnp.where(last_tp, 1, 0), sp_size),
        lax.rem(tp + 1, tp_size),
    )
    prv = (
        lax.rem(sp + sp_size - jnp.where(first_tp, 1, 0), sp_size),
        lax.rem(tp + tp_size - 1, tp_size),
    )
    me = sp * tp_size + tp
    total = sp_size * tp_size
    inv_root = HEAD_DIM**-0.5

    def loads(k):
        ahead, back = k, HEADS - 1 - k
        places = [
            (k_hbm, kv.at[ahead, 0, pl.ds(512, ROWS)], ahead),
            (v_hbm, kv.at[ahead, 1, pl.ds(512, ROWS)], ahead),
            (q_hbm, qg.at[back, 0, pl.ds(0, ROWS)], back),
            (g_hbm, qg.at[back, 1, pl.ds(0, ROWS)], back),
        ]
        return [
            pltpu.make_async_copy(
                src.at[:, pl.ds(pl.multiple_of(h * HEAD_DIM, HEAD_DIM), HEAD_DIM)],
                dst,
                load_sem.at[n, h],
            )
            for n, (src, dst, h) in enumerate(places)
        ]

    def stores(k):
        ahead, back = k, HEADS - 1 - k
        return [
            pltpu.make_async_copy(
                outs.at[n, h],
                out.at[:, pl.ds(pl.multiple_of(h * HEAD_DIM, HEAD_DIM), HEAD_DIM)],
                out_sem.at[n, h],
            )
            for n, (out, h) in enumerate(((dq_hbm, ahead), (dk_hbm, back), (dv_hbm, back)))
        ]

    def kv_copy(h, lag):
        src, dst = (512, 256) if lag == 0 else (256, 0)
        return pltpu.make_async_remote_copy(
            src_ref=kv.at[h, :, pl.ds(src, ROWS)],
            dst_ref=kv.at[h, :, pl.ds(dst, ROWS)],
            send_sem=kv_send.at[lag, h],
            recv_sem=kv_recv.at[lag, h],
            device_id=nxt,
            device_id_type=MESH,
        )

    def qg_copy(h, lag):
        return pltpu.make_async_remote_copy(
            src_ref=qg.at[h, :, pl.ds(lag * ROWS, ROWS)],
            dst_ref=qg.at[h, :, pl.ds((lag + 1) * ROWS, ROWS)],
            send_sem=qg_send.at[lag, h],
            recv_sem=qg_recv.at[lag, h],
            device_id=prv,
            device_id_type=MESH,
        )

    def st_copy(lag):
        return pltpu.make_async_remote_copy(
            src_ref=stats.at[lag],
            dst_ref=stats.at[lag + 1],
            send_sem=st_send.at[lag],
            recv_sem=st_recv.at[lag],
            device_id=prv,
            device_id_type=MESH,
        )

    stat_loads = [
        pltpu.make_async_copy(lse_hbm, stats.at[0, pl.ds(0, HEADS)], stat_sem.at[0]),
        pltpu.make_async_copy(dot_hbm, stats.at[0, pl.ds(HEADS, HEADS)], stat_sem.at[1]),
    ]

    barrier = pltpu.get_barrier_semaphore()
    for neighbour in (nxt, prv):
        pl.semaphore_signal(barrier, inc=1, device_id=neighbour, device_id_type=MESH)

    for copy in stat_loads:
        copy.start()

    @pl.loop(0, HEADS)
    def _(k):
        for copy in loads(k):
            copy.start()

    pl.semaphore_wait(barrier, 2)

    def await_loads(k):
        for copy in loads(k):
            copy.wait()

    def send_own(k):
        kv_copy(k, 0).start()
        qg_copy(HEADS - 1 - k, 0).start()

    for copy in stat_loads:
        copy.wait()
    st_copy(0).start()
    for k in range(2):
        await_loads(k)
        send_own(k)
    pl.loop(2, HEADS)(await_loads)

    ext[...] = jnp.broadcast_to(table_ref[:, TABLE_LEN - 1 : TABLE_LEN], (HEADS, 512))
    ext[:, 0:TABLE_LEN] = table_ref[...]
    ext[...] = pltpu.roll(ext[...], 65, 1) * LOG2E
    key_row = lax.broadcasted_iota(jnp.int32, (HALF, HALF), 0)
    query_col = lax.broadcasted_iota(jnp.int32, (HALF, HALF), 1)
    near_off = (key_row >= SEG_LEN) & (query_col < SEG_LEN)
    far_off = (key_row < SEG_LEN) & (query_col >= SEG_LEN)

    @pl.loop(0, HEADS)
    def _(h):
        row = ext[pl.ds(h, 1), :]
        for d in range(3):
            low = row[:, HALF * d : HALF * (d + 1)]
            high = row[:, HALF * (d + 1) : HALF * (d + 2)]
            around = jnp.broadcast_to(jnp.concatenate([high, low], axis=1), (HALF, 2 * HALF))
            tile = pltpu.roll(around, 0, 1, stride=1, stride_axis=0)[:, :HALF]
            if d == 0:
                tile = jnp.where(near_off, -FAR, tile)
            bias[h, d] = tile
        flat = jnp.broadcast_to(row[:, 511:512], (HALF, HALF))
        bias[h, 3] = flat
        bias[h, 4] = jnp.where(far_off, -FAR, flat)

    st_copy(0).wait_recv()
    st_copy(1).start()
    st_copy(1).wait_recv()

    def off(cond):
        return jnp.where(cond, FAR, 0.0).astype(F32)

    key_off = [off(me < 0), off(me < 1), off(me < 2)]
    query_off = [off(me < 0), off(me + 1 >= total), off(me + 2 >= total)]
    for lag in range(3):
        for n in range(2 * HEADS):
            row = stats[lag, n : n + 1, :]
            if n < HEADS:
                row = row * LOG2E + query_off[lag]
            wide[lag, n] = jnp.broadcast_to(row, (8, ROWS))

    def tile_terms(scores, weight_grads, bias_tile, log_row, dot_row):
        weights = jnp.exp2(scores * (inv_root * LOG2E) + (bias_tile - log_row))
        return weights, weights * (weight_grads - dot_row)

    def add_to(side, part, d, score_grads):
        if part == 0:
            acc[side, d] = score_grads
        else:
            acc[side, d] += score_grads

    def query_side(h):
        for part in range(2):
            rows = pl.ds(part * HALF, HALF)
            queries, grads = qg[h, 0, rows, :], qg[h, 1, rows, :]
            keys = kv[h, 0, pl.ds(part * HALF, BAND), :]
            values = kv[h, 1, pl.ds(part * HALF, BAND), :]
            scores = dot_nt(keys, queries)
            weight_grads = dot_nt(values, grads)
            log_row = wide[0, h, 0:1, rows]
            dot_row = wide[0, HEADS + h, 0:1, rows]
            pieces = []
            for t in range(5):
                d, lag = 4 - t, 2 - (part + t) // 2
                cut = slice(t * HALF, (t + 1) * HALF)
                _, score_grads = tile_terms(
                    scores[cut], weight_grads[cut], bias[h, d], log_row + key_off[lag], dot_row
                )
                add_to(0, part, d, score_grads)
                pieces.append(score_grads.astype(BF16))
            total_grads = dot_tn(jnp.concatenate(pieces, axis=0), keys)
            outs[0, h, rows, :] = (total_grads * inv_root).astype(BF16)

    def key_side(h):
        for part in range(2):
            rows = pl.ds(part * HALF, HALF)
            own = pl.ds(512 + part * HALF, HALF)
            keys, values = kv[h, 0, own, :], kv[h, 1, own, :]
            queries = qg[h, 0, pl.ds(part * HALF, BAND), :]
            grads = qg[h, 1, pl.ds(part * HALF, BAND), :]
            scores = dot_nt(keys, queries)
            weight_grads = dot_nt(values, grads)
            score_pieces, weight_pieces = [], []
            for d in range(5):
                lag, cols = (part + d) // 2, pl.ds((part + d) % 2 * HALF, HALF)
                cut = slice(d * HALF, (d + 1) * HALF)
                log_row = wide[lag, h, 0:1, cols]
                dot_row = wide[lag, HEADS + h, 0:1, cols]
                weights, score_grads = tile_terms(
                    scores[:, cut], weight_grads[:, cut], bias[h, d], log_row, dot_row
                )
                add_to(1, part, d, score_grads)
                score_pieces.append(score_grads.astype(BF16))
                weight_pieces.append(weights.astype(BF16))
            key_grads = dot_nn(jnp.concatenate(score_pieces, axis=1), queries)
            outs[1, h, rows, :] = (key_grads * inv_root).astype(BF16)
            value_grads = dot_nn(jnp.concatenate(weight_pieces, axis=1), grads)
            outs[2, h, rows, :] = value_grads.astype(BF16)

    def table_row(side, h):
        zeros = jnp.zeros((HALF, HALF), F32)
        part = jnp.concatenate([acc[side, 0], acc[side, 1], acc[side, 2], zeros], axis=1)
        for step in (64, 32, 16, 8):
            part = part[:step] + pltpu.roll(part[step:], 512 - step, 1)
        row_id = lax.broadcasted_iota(jnp.int32, (8, 512), 0)
        for step in (4, 2, 1):
            moved = pltpu.roll(part, 512 - step, 1)
            part = jnp.where((row_id & step) != 0, moved, part)
        far = jnp.sum(acc[side, 3] + acc[side, 4], keepdims=True)
        by_distance = pltpu.roll(jnp.sum(part, axis=0, keepdims=True), SEG_LEN - 1, 1)
        lane = lax.broadcasted_iota(jnp.int32, (1, 512), 1)
        top = TABLE_LEN - 1
        clipped = (lane >= top) & (lane < 448)
        far = far + jnp.sum(jnp.where(clipped, by_distance, 0.0), keepdims=True)
        row = jnp.where(lane < top, by_distance, jnp.where(lane == top, far, 0.0))
        gt_ref[pl.ds(h, 1), :] = row

    @pl.loop(0, HEADS + 1)
    def _(k):
        @pl.when(k < HEADS)
        def _():
            kv_copy(k, 0).wait_recv()
            kv_copy(k, 1).start()
            qg_copy(HEADS - 1 - k, 0).wait_recv()
            qg_copy(HEADS - 1 - k, 1).start()

        @pl.when(k < HEADS - 2)
        def _():
            send_own(k + 2)

        @pl.when(k >= 1)
        def _():
            ahead, back = k - 1, HEADS - k
            kv_copy(ahead, 1).wait_recv()
            query_side(ahead)
            qg_copy(back, 1).wait_recv()
            key_side(back)

            @pl.when(k <= HEADS // 2)
            def _():
                table_row(0, ahead)
                table_row(1, back)

            for copy in stores(ahead):
                copy.start()

    @pl.loop(0, HEADS)
    def _(h):
        for lag in range(2):
            kv_copy(h, lag).wait_send()
            qg_copy(h, lag).wait_send()
        for copy in stores(h):
            copy.wait()

    st_copy(0).wait_send()
    st_copy(1).wait_send()


def solution(mesh):
    sp_size, tp_size = mesh.shape["sp"], mesh.shape["tp"]

    def local(query_rows, key_rows, value_rows, out_grad, log_totals, out_dot, bias_table):
        hbm = pl.BlockSpec(memory_space=pl.ANY)
        vmem = pl.BlockSpec(memory_space=pltpu.VMEM)
        rows = jax.ShapeDtypeStruct(query_rows.shape, BF16)
        grad_query, grad_key, grad_value, table_part = pl.pallas_call(
            functools.partial(kernel, sp_size, tp_size),
            out_shape=(rows, rows, rows, jax.ShapeDtypeStruct((HEADS, 512), F32)),
            in_specs=[hbm] * 6 + [vmem],
            out_specs=(hbm, hbm, hbm, vmem),
            scratch_shapes=[
                pltpu.VMEM((HEADS, 2, 3 * ROWS, HEAD_DIM), BF16),
                pltpu.VMEM((HEADS, 2, 3 * ROWS, HEAD_DIM), BF16),
                pltpu.VMEM((3, 2 * HEADS, ROWS), F32),
                pltpu.VMEM((3, 2 * HEADS, 8, ROWS), F32),
                pltpu.VMEM((HEADS, 5, HALF, HALF), F32),
                pltpu.VMEM((HEADS, 512), F32),
                pltpu.VMEM((2, 5, HALF, HALF), F32),
                pltpu.VMEM((3, HEADS, ROWS, HEAD_DIM), BF16),
                pltpu.SemaphoreType.DMA((4, HEADS)),
                pltpu.SemaphoreType.DMA((2,)),
                pltpu.SemaphoreType.DMA((3, HEADS)),
                pltpu.SemaphoreType.DMA((2, HEADS)),
                pltpu.SemaphoreType.DMA((2, HEADS)),
                pltpu.SemaphoreType.DMA((2, HEADS)),
                pltpu.SemaphoreType.DMA((2, HEADS)),
                pltpu.SemaphoreType.DMA((2,)),
                pltpu.SemaphoreType.DMA((2,)),
            ],
            compiler_params=pltpu.CompilerParams(
                collective_id=0, has_side_effects=True
            ),
        )(query_rows, key_rows, value_rows, out_grad, log_totals.T, out_dot.T, bias_table)
        grad_table = lax.psum(table_part[:, :TABLE_LEN], ("sp", "tp"))
        return grad_query, grad_key, grad_value, grad_table

    split = P(("sp", "tp"), None)
    return jax.shard_map(
        local,
        mesh=mesh,
        in_specs=(split,) * 6 + (P(),),
        out_specs=(split, split, split, P()),
        check_vma=False,
    )
```

```python
import functools
import math

import jax
import jax.numpy as jnp
from jax import lax
from jax.experimental import pallas as pl
from jax.experimental.pallas import tpu as pltpu
from jax.sharding import PartitionSpec as P

SEG_LEN = 64
REL_CLIP = 256
ROWS = 256
HALF = 128
BAND = 640
HEADS = 8
HEAD_DIM = 128
TABLE_LEN = 320
LOG2E = math.log2(math.e)
FAR = 1e30
SP_SHAPE = (12, 8, 2)
GROUP = HEADS // 2
MESH = pl.DeviceIdType.MESH
F32 = jnp.float32
BF16 = jnp.bfloat16


def dot_nt(lhs, rhs):
    return lax.dot_general(lhs, rhs, (((1,), (1,)), ((), ())), preferred_element_type=F32)


def dot_nn(lhs, rhs):
    return lax.dot_general(lhs, rhs, (((1,), (0,)), ((), ())), preferred_element_type=F32)


def dot_tn(lhs, rhs):
    return lax.dot_general(lhs, rhs, (((0,), (0,)), ((), ())), preferred_element_type=F32)


def kernel(
    sp_size,
    tp_size,
    q_hbm,
    k_hbm,
    v_hbm,
    g_hbm,
    lse_hbm,
    dot_hbm,
    table_ref,
    dq_ref,
    dk_ref,
    dv_ref,
    gt_ref,
    kv,
    qg,
    stats,
    wide,
    bias,
    ext,
    acc,
    tab,
    tab_core,
    tab_y,
    tab_z,
    tab_x,
    tab_all,
    load_sem,
    stat_sem,
    core_sem,
    y_send,
    y_recv,
    z_send,
    z_recv,
    x_send,
    x_recv,
    all_send,
    all_recv,
    kv_send,
    kv_recv,
    qg_send,
    qg_recv,
    st_send,
    st_recv,
):
    sp, tp = lax.axis_index("sp"), lax.axis_index("tp")
    last_tp, first_tp = tp == tp_size - 1, tp == 0
    nxt = (
        lax.rem(sp + jnp.where(last_tp, 1, 0), sp_size),
        lax.rem(tp + 1, tp_size),
    )
    prv = (
        lax.rem(sp + sp_size - jnp.where(first_tp, 1, 0), sp_size),
        lax.rem(tp + tp_size - 1, tp_size),
    )
    z_size, y_size, core_size = SP_SHAPE
    at_z, at_y, at_core = sp // (y_size * core_size), sp // core_size % y_size, sp % core_size

    def at(z, y, core):
        return ((z * y_size + y) * core_size + core, tp)

    me = sp * tp_size + tp
    total = sp_size * tp_size
    inv_root = HEAD_DIM**-0.5

    def cols_of(h):
        return pl.ds(pl.multiple_of(h * HEAD_DIM, HEAD_DIM), HEAD_DIM)

    def loads(k):
        ahead, back = k, HEADS - 1 - k
        places = [
            (k_hbm, kv.at[ahead, 0, pl.ds(512, ROWS)], ahead),
            (v_hbm, kv.at[ahead, 1, pl.ds(512, ROWS)], ahead),
            (q_hbm, qg.at[back, 0, pl.ds(0, ROWS)], back),
            (g_hbm, qg.at[back, 1, pl.ds(0, ROWS)], back),
        ]
        return [
            pltpu.make_async_copy(
                src.at[:, cols_of(h)],
                dst,
                load_sem.at[n, h],
            )
            for n, (src, dst, h) in enumerate(places)
        ]

    def kv_copy(h, lag):
        src, dst = (512, 256) if lag == 0 else (256, 0)
        return pltpu.make_async_remote_copy(
            src_ref=kv.at[h, :, pl.ds(src, ROWS)],
            dst_ref=kv.at[h, :, pl.ds(dst, ROWS)],
            send_sem=kv_send.at[lag, h],
            recv_sem=kv_recv.at[lag, h],
            device_id=nxt,
            device_id_type=MESH,
        )

    def qg_copy(h, lag):
        return pltpu.make_async_remote_copy(
            src_ref=qg.at[h, :, pl.ds(lag * ROWS, ROWS)],
            dst_ref=qg.at[h, :, pl.ds((lag + 1) * ROWS, ROWS)],
            send_sem=qg_send.at[lag, h],
            recv_sem=qg_recv.at[lag, h],
            device_id=prv,
            device_id_type=MESH,
        )

    def st_copy(lag):
        return pltpu.make_async_remote_copy(
            src_ref=stats.at[lag],
            dst_ref=stats.at[lag + 1],
            send_sem=st_send.at[lag],
            recv_sem=st_recv.at[lag],
            device_id=prv,
            device_id_type=MESH,
        )

    class Exchange:
        def __init__(self, slots, size, mine, device, send, recv):
            self.slots, self.size, self.mine = slots, size, mine
            self.device, self.send, self.recv = device, send, recv

        def other(self, step):
            return lax.rem(self.mine + step, self.size)

        def copy(self, step, slot):
            return pltpu.make_async_remote_copy(
                src_ref=self.slots.at[slot],
                dst_ref=self.slots.at[slot],
                send_sem=self.send.at[step],
                recv_sem=self.recv.at[slot],
                device_id=self.device(self.other(step)),
                device_id_type=MESH,
            )

        def greet(self):
            @pl.loop(1, self.size)
            def _(step):
                pl.semaphore_signal(
                    barrier, inc=1, device_id=self.device(self.other(step)), device_id_type=MESH
                )

        def start(self, value):
            self.slots[self.mine] = value

            @pl.loop(1, self.size)
            def _(step):
                self.copy(step, self.mine).start()

        def receive(self):
            @pl.loop(1, self.size)
            def _(step):
                self.copy(step, self.other(step)).wait_recv()

        def total(self):
            self.receive()
            value = self.slots[0]
            for slot in range(1, self.size):
                value = value + self.slots[slot]
            return value

        def finish(self):
            @pl.loop(1, self.size)
            def _(step):
                self.copy(step, self.mine).wait_send()

    over_y = Exchange(tab_y, y_size, at_y, lambda y: at(at_z, y, at_core), y_send, y_recv)
    over_z = Exchange(tab_z, z_size, at_z, lambda z: at(z, at_y, at_core), z_send, z_recv)
    over_x = Exchange(tab_x, tp_size, tp, lambda x: (sp, x), x_send, x_recv)
    other_core = at(at_z, at_y, 1 - at_core)
    over_cores = Exchange(
        tab_all, core_size, at_core, lambda core: at(at_z, at_y, core), all_send, all_recv
    )
    core_copy = pltpu.make_async_remote_copy(
        src_ref=tab.at[pl.ds((1 - at_core) * GROUP, GROUP)],
        dst_ref=tab_core,
        send_sem=core_sem.at[0],
        recv_sem=core_sem.at[1],
        device_id=other_core,
        device_id_type=MESH,
    )

    stat_loads = [
        pltpu.make_async_copy(lse_hbm, stats.at[0, pl.ds(0, HEADS)], stat_sem.at[0]),
        pltpu.make_async_copy(dot_hbm, stats.at[0, pl.ds(HEADS, HEADS)], stat_sem.at[1]),
    ]

    barrier = pltpu.get_barrier_semaphore()
    for neighbour in (nxt, prv):
        pl.semaphore_signal(barrier, inc=1, device_id=neighbour, device_id_type=MESH)
    for line in (over_z, over_y, over_x, over_cores):
        line.greet()

    for copy in stat_loads:
        copy.start()

    @pl.loop(0, HEADS)
    def _(k):
        for copy in loads(k):
            copy.start()

    ext[...] = jnp.broadcast_to(table_ref[:, TABLE_LEN - 1 : TABLE_LEN], (HEADS, 512))
    ext[:, 0:TABLE_LEN] = table_ref[...]
    ext[...] = pltpu.roll(ext[...], 65, 1) * LOG2E
    key_row = lax.broadcasted_iota(jnp.int32, (HALF, HALF), 0)
    query_col = lax.broadcasted_iota(jnp.int32, (HALF, HALF), 1)
    near_off = (key_row >= SEG_LEN) & (query_col < SEG_LEN)
    far_off = (key_row < SEG_LEN) & (query_col >= SEG_LEN)

    @pl.loop(0, HEADS)
    def _(h):
        row = ext[pl.ds(h, 1), :]
        for d in range(3):
            low = row[:, HALF * d : HALF * (d + 1)]
            high = row[:, HALF * (d + 1) : HALF * (d + 2)]
            around = jnp.broadcast_to(jnp.concatenate([high, low], axis=1), (HALF, 2 * HALF))
            tile = pltpu.roll(around, 0, 1, stride=1, stride_axis=0)[:, :HALF]
            if d == 0:
                tile = jnp.where(near_off, -FAR, tile)
            bias[h, d] = tile
        flat = jnp.broadcast_to(row[:, 511:512], (HALF, HALF))
        bias[h, 3] = flat
        bias[h, 4] = jnp.where(far_off, -FAR, flat)

    pl.semaphore_wait(barrier, z_size + y_size + tp_size + core_size - 2)

    def await_loads(k):
        for copy in loads(k):
            copy.wait()

    def send_own(k):
        kv_copy(k, 0).start()
        qg_copy(HEADS - 1 - k, 0).start()

    for copy in stat_loads:
        copy.wait()
    st_copy(0).start()
    for k in range(2):
        await_loads(k)
        send_own(k)
    pl.loop(2, HEADS)(await_loads)

    st_copy(0).wait_recv()
    st_copy(1).start()
    st_copy(1).wait_recv()

    def off(cond):
        return jnp.where(cond, FAR, 0.0).astype(F32)

    key_off = [off(me < 0), off(me < 1), off(me < 2)]
    query_off = [off(me < 0), off(me + 1 >= total), off(me + 2 >= total)]
    for lag in range(3):
        for n in range(2 * HEADS):
            row = stats[lag, n : n + 1, :]
            if n < HEADS:
                row = row * LOG2E + query_off[lag]
            wide[lag, n] = jnp.broadcast_to(row, (8, ROWS))

    def tile_terms(scores, weight_grads, bias_tile, log_row, dot_row):
        weights = jnp.exp2(scores * (inv_root * LOG2E) + (bias_tile - log_row))
        return weights, weights * (weight_grads - dot_row)

    def add_to(side, part, d, score_grads):
        if part == 0:
            acc[side, d] = score_grads
        else:
            acc[side, d] += score_grads

    def query_side(h):
        for part in range(2):
            rows = pl.ds(part * HALF, HALF)
            queries, grads = qg[h, 0, rows, :], qg[h, 1, rows, :]
            keys = kv[h, 0, pl.ds(part * HALF, BAND), :]
            values = kv[h, 1, pl.ds(part * HALF, BAND), :]
            scores = dot_nt(keys, queries)
            weight_grads = dot_nt(values, grads)
            log_row = wide[0, h, 0:1, rows]
            dot_row = wide[0, HEADS + h, 0:1, rows]
            pieces = []
            for t in range(5):
                d, lag = 4 - t, 2 - (part + t) // 2
                cut = slice(t * HALF, (t + 1) * HALF)
                _, score_grads = tile_terms(
                    scores[cut], weight_grads[cut], bias[h, d], log_row + key_off[lag], dot_row
                )
                add_to(0, part, d, score_grads)
                pieces.append(score_grads.astype(BF16))
            total_grads = dot_tn(jnp.concatenate(pieces, axis=0), keys)
            dq_ref[rows, cols_of(h)] = (total_grads * inv_root).astype(BF16)

    def key_side(h):
        for part in range(2):
            rows = pl.ds(part * HALF, HALF)
            own = pl.ds(512 + part * HALF, HALF)
            keys, values = kv[h, 0, own, :], kv[h, 1, own, :]
            queries = qg[h, 0, pl.ds(part * HALF, BAND), :]
            grads = qg[h, 1, pl.ds(part * HALF, BAND), :]
            scores = dot_nt(keys, queries)
            weight_grads = dot_nt(values, grads)
            score_pieces, weight_pieces = [], []
            for d in range(5):
                lag, cols = (part + d) // 2, pl.ds((part + d) % 2 * HALF, HALF)
                cut = slice(d * HALF, (d + 1) * HALF)
                log_row = wide[lag, h, 0:1, cols]
                dot_row = wide[lag, HEADS + h, 0:1, cols]
                weights, score_grads = tile_terms(
                    scores[:, cut], weight_grads[:, cut], bias[h, d], log_row, dot_row
                )
                add_to(1, part, d, score_grads)
                score_pieces.append(score_grads.astype(BF16))
                weight_pieces.append(weights.astype(BF16))
            key_grads = dot_nn(jnp.concatenate(score_pieces, axis=1), queries)
            dk_ref[rows, cols_of(h)] = (key_grads * inv_root).astype(BF16)
            value_grads = dot_nn(jnp.concatenate(weight_pieces, axis=1), grads)
            dv_ref[rows, cols_of(h)] = value_grads.astype(BF16)

    def table_row(side, h):
        zeros = jnp.zeros((HALF, HALF), F32)
        part = jnp.concatenate([acc[side, 0], acc[side, 1], acc[side, 2], zeros], axis=1)
        for step in (64, 32, 16, 8):
            part = part[:step] + pltpu.roll(part[step:], 512 - step, 1)
        row_id = lax.broadcasted_iota(jnp.int32, (8, 512), 0)
        for step in (4, 2, 1):
            moved = pltpu.roll(part, 512 - step, 1)
            part = jnp.where((row_id & step) != 0, moved, part)
        far = jnp.sum(acc[side, 3] + acc[side, 4], keepdims=True)
        by_distance = pltpu.roll(jnp.sum(part, axis=0, keepdims=True), SEG_LEN - 1, 1)
        lane = lax.broadcasted_iota(jnp.int32, (1, 512), 1)
        top = TABLE_LEN - 1
        clipped = (lane >= top) & (lane < 448)
        far = far + jnp.sum(jnp.where(clipped, by_distance, 0.0), keepdims=True)
        row = jnp.where(lane < top, by_distance, jnp.where(lane == top, far, 0.0))
        for n in range(4):
            tab[h, n : n + 1, :] = row[:, n * HALF : (n + 1) * HALF]

    @pl.loop(0, HEADS + 1)
    def _(k):
        @pl.when(k < HEADS)
        def _():
            kv_copy(k, 0).wait_recv()
            kv_copy(k, 1).start()
            qg_copy(HEADS - 1 - k, 0).wait_recv()
            qg_copy(HEADS - 1 - k, 1).start()

        @pl.when(k < HEADS - 2)
        def _():
            send_own(k + 2)

        @pl.when(k >= 1)
        def _():
            ahead, back = k - 1, HEADS - k
            kv_copy(ahead, 1).wait_recv()
            query_side(ahead)

            @pl.when(k == 5)
            def _():
                core_copy.wait_recv()
                over_y.start(tab[pl.ds(at_core * GROUP, GROUP)] + tab_core[...])

            @pl.when(k == 6)
            def _():
                over_z.start(over_y.total())

            @pl.when(k == 7)
            def _():
                over_x.start(over_z.total())

            @pl.when(k == 8)
            def _():
                over_cores.start(over_x.total())

            qg_copy(back, 1).wait_recv()
            key_side(back)

            @pl.when(k <= HEADS // 2)
            def _():
                table_row(0, ahead)
                table_row(1, back)

            @pl.when(k == HEADS // 2)
            def _():
                core_copy.start()

    over_cores.receive()
    for h in range(HEADS):
        for n in range(3):
            width = min(HALF, TABLE_LEN - n * HALF)
            gt_ref[h : h + 1, n * HALF : n * HALF + width] = tab_all[
                h // GROUP, h % GROUP, n : n + 1, :width
            ]

    @pl.loop(0, HEADS)
    def _(h):
        for lag in range(2):
            kv_copy(h, lag).wait_send()
            qg_copy(h, lag).wait_send()

    st_copy(0).wait_send()
    st_copy(1).wait_send()
    core_copy.wait_send()
    for line in (over_y, over_z, over_x, over_cores):
        line.finish()


def solution(mesh):
    sp_size, tp_size = mesh.shape["sp"], mesh.shape["tp"]

    def local(query_rows, key_rows, value_rows, out_grad, log_totals, out_dot, bias_table):
        hbm = pl.BlockSpec(memory_space=pltpu.HBM)
        z_size, y_size, core_size = SP_SHAPE
        tiles = (GROUP, 4, HALF)
        vmem = pl.BlockSpec(memory_space=pltpu.VMEM)
        rows = jax.ShapeDtypeStruct(query_rows.shape, BF16)
        return pl.pallas_call(
            functools.partial(kernel, sp_size, tp_size),
            out_shape=(rows, rows, rows, jax.ShapeDtypeStruct(bias_table.shape, F32)),
            in_specs=[hbm] * 6 + [vmem],
            out_specs=(vmem, vmem, vmem, vmem),
            scratch_shapes=[
                pltpu.VMEM((HEADS, 2, 3 * ROWS, HEAD_DIM), BF16),
                pltpu.VMEM((HEADS, 2, 3 * ROWS, HEAD_DIM), BF16),
                pltpu.VMEM((3, 2 * HEADS, ROWS), F32),
                pltpu.VMEM((3, 2 * HEADS, 8, ROWS), F32),
                pltpu.VMEM((HEADS, 5, HALF, HALF), F32),
                pltpu.VMEM((HEADS, 512), F32),
                pltpu.VMEM((2, 5, HALF, HALF), F32),
                pltpu.VMEM((HEADS, 4, HALF), F32),
                pltpu.VMEM(tiles, F32),
                pltpu.VMEM((y_size,) + tiles, F32),
                pltpu.VMEM((z_size,) + tiles, F32),
                pltpu.VMEM((tp_size,) + tiles, F32),
                pltpu.VMEM((core_size,) + tiles, F32),
                pltpu.SemaphoreType.DMA((4, HEADS)),
                pltpu.SemaphoreType.DMA((2,)),
                pltpu.SemaphoreType.DMA((2,)),
                pltpu.SemaphoreType.DMA((y_size,)),
                pltpu.SemaphoreType.DMA((y_size,)),
                pltpu.SemaphoreType.DMA((z_size,)),
                pltpu.SemaphoreType.DMA((z_size,)),
                pltpu.SemaphoreType.DMA((tp_size,)),
                pltpu.SemaphoreType.DMA((tp_size,)),
                pltpu.SemaphoreType.DMA((core_size,)),
                pltpu.SemaphoreType.DMA((core_size,)),
                pltpu.SemaphoreType.DMA((2, HEADS)),
                pltpu.SemaphoreType.DMA((2, HEADS)),
                pltpu.SemaphoreType.DMA((2, HEADS)),
                pltpu.SemaphoreType.DMA((2, HEADS)),
                pltpu.SemaphoreType.DMA((2,)),
                pltpu.SemaphoreType.DMA((2,)),
            ],
            compiler_params=pltpu.CompilerParams(
                collective_id=0, has_side_effects=True, vmem_limit_bytes=32 * 2**20
            ),
        )(query_rows, key_rows, value_rows, out_grad, log_totals.T, out_dot.T, bias_table)

    split = P(("sp", "tp"), None)
    return jax.shard_map(
        local,
        mesh=mesh,
        in_specs=(split,) * 6 + (P(),),
        out_specs=(split, split, split, P()),
        check_vma=False,
    )
```

```python
import functools
import math

import jax
import jax.numpy as jnp
from jax import lax
from jax.experimental import pallas as pl
from jax.experimental.pallas import tpu as pltpu
from jax.sharding import PartitionSpec as P

SEG_LEN = 64
REL_CLIP = 256
ROWS = 256
HALF = 128
BAND = 640
HEADS = 8
HEAD_DIM = 128
TABLE_LEN = 320
LOG2E = math.log2(math.e)
FAR = 1e30
SP_SHAPE = (12, 8, 2)
GROUP = HEADS // 2
MESH = pl.DeviceIdType.MESH
F32 = jnp.float32
BF16 = jnp.bfloat16


def dot_nt(lhs, rhs):
    return lax.dot_general(lhs, rhs, (((1,), (1,)), ((), ())), preferred_element_type=F32)


def dot_nn(lhs, rhs):
    return lax.dot_general(lhs, rhs, (((1,), (0,)), ((), ())), preferred_element_type=F32)


def dot_tn(lhs, rhs):
    return lax.dot_general(lhs, rhs, (((0,), (0,)), ((), ())), preferred_element_type=F32)


def kernel(
    sp_size,
    tp_size,
    q_hbm,
    k_hbm,
    v_hbm,
    g_hbm,
    lse_hbm,
    dot_hbm,
    table_hbm,
    dq_ref,
    dk_ref,
    dv_ref,
    gt_ref,
    kv,
    qg,
    stats,
    wide,
    bias,
    table_ref,
    ext,
    acc,
    tab,
    tab_core,
    tab_y,
    tab_z,
    tab_x,
    tab_all,
    load_sem,
    stat_sem,
    chain,
    core_sem,
    y_send,
    y_recv,
    z_send,
    z_recv,
    x_send,
    x_recv,
    all_send,
    all_recv,
    kv_send,
    kv_recv,
    qg_send,
    qg_recv,
    st_send,
    st_recv,
):
    sp, tp = lax.axis_index("sp"), lax.axis_index("tp")
    last_tp, first_tp = tp == tp_size - 1, tp == 0
    nxt = (
        lax.rem(sp + jnp.where(last_tp, 1, 0), sp_size),
        lax.rem(tp + 1, tp_size),
    )
    prv = (
        lax.rem(sp + sp_size - jnp.where(first_tp, 1, 0), sp_size),
        lax.rem(tp + tp_size - 1, tp_size),
    )
    z_size, y_size, core_size = SP_SHAPE
    at_z, at_y, at_core = sp // (y_size * core_size), sp // core_size % y_size, sp % core_size

    def at(z, y, core):
        return ((z * y_size + y) * core_size + core, tp)

    me = sp * tp_size + tp
    total = sp_size * tp_size
    inv_root = HEAD_DIM**-0.5

    def cols_of(h):
        return pl.ds(pl.multiple_of(h * HEAD_DIM, HEAD_DIM), HEAD_DIM)

    def loads(k):
        ahead, back = k, HEADS - 1 - k
        places = [
            (k_hbm, kv.at[ahead, 0, pl.ds(512, ROWS)], ahead),
            (v_hbm, kv.at[ahead, 1, pl.ds(512, ROWS)], ahead),
            (q_hbm, qg.at[back, 0, pl.ds(0, ROWS)], back),
            (g_hbm, qg.at[back, 1, pl.ds(0, ROWS)], back),
        ]
        return [
            pltpu.make_async_copy(
                src.at[:, cols_of(h)],
                dst,
                load_sem.at[n, h],
            )
            for n, (src, dst, h) in enumerate(places)
        ]

    def kv_copy(h, lag):
        src, dst = (512, 256) if lag == 0 else (256, 0)
        return pltpu.make_async_remote_copy(
            src_ref=kv.at[h, :, pl.ds(src, ROWS)],
            dst_ref=kv.at[h, :, pl.ds(dst, ROWS)],
            send_sem=kv_send.at[lag, h],
            recv_sem=kv_recv.at[lag, h],
            device_id=nxt,
            device_id_type=MESH,
        )

    def qg_copy(h, lag):
        return pltpu.make_async_remote_copy(
            src_ref=qg.at[h, :, pl.ds(lag * ROWS, ROWS)],
            dst_ref=qg.at[h, :, pl.ds((lag + 1) * ROWS, ROWS)],
            send_sem=qg_send.at[lag, h],
            recv_sem=qg_recv.at[lag, h],
            device_id=prv,
            device_id_type=MESH,
        )

    def st_copy(lag):
        return pltpu.make_async_remote_copy(
            src_ref=stats.at[lag],
            dst_ref=stats.at[lag + 1],
            send_sem=st_send.at[lag],
            recv_sem=st_recv.at[lag],
            device_id=prv,
            device_id_type=MESH,
        )

    class Exchange:
        def __init__(self, slots, size, mine, device, send, recv):
            self.slots, self.size, self.mine = slots, size, mine
            self.device, self.send, self.recv = device, send, recv

        def other(self, step):
            return lax.rem(self.mine + step, self.size)

        def copy(self, step, slot):
            return pltpu.make_async_remote_copy(
                src_ref=self.slots.at[slot],
                dst_ref=self.slots.at[slot],
                send_sem=self.send.at[step],
                recv_sem=self.recv.at[slot],
                device_id=self.device(self.other(step)),
                device_id_type=MESH,
            )

        def start(self, value):
            self.slots[self.mine] = value

            @pl.loop(1, self.size)
            def _(step):
                self.copy(step, self.mine).start()

        def receive(self):
            @pl.loop(1, self.size)
            def _(step):
                self.copy(step, self.other(step)).wait_recv()

        def total(self):
            self.receive()
            value = self.slots[0]
            for slot in range(1, self.size):
                value = value + self.slots[slot]
            return value

        def finish(self):
            @pl.loop(1, self.size)
            def _(step):
                self.copy(step, self.mine).wait_send()

    over_y = Exchange(tab_y, y_size, at_y, lambda y: at(at_z, y, at_core), y_send, y_recv)
    over_z = Exchange(tab_z, z_size, at_z, lambda z: at(z, at_y, at_core), z_send, z_recv)
    over_x = Exchange(tab_x, tp_size, tp, lambda x: (sp, x), x_send, x_recv)
    other_core = at(at_z, at_y, 1 - at_core)
    over_cores = Exchange(
        tab_all, core_size, at_core, lambda core: at(at_z, at_y, core), all_send, all_recv
    )
    core_copy = pltpu.make_async_remote_copy(
        src_ref=tab.at[pl.ds((1 - at_core) * GROUP, GROUP)],
        dst_ref=tab_core,
        send_sem=core_sem.at[0],
        recv_sem=core_sem.at[1],
        device_id=other_core,
        device_id_type=MESH,
    )

    stat_loads = [
        pltpu.make_async_copy(lse_hbm, stats.at[0, pl.ds(0, HEADS)], stat_sem.at[0]),
        pltpu.make_async_copy(dot_hbm, stats.at[0, pl.ds(HEADS, HEADS)], stat_sem.at[1]),
    ]
    table_load = pltpu.make_async_copy(table_hbm, table_ref, stat_sem.at[2])

    has_prv, has_nxt = me >= 1, me + 1 < total
    has_prv2, has_nxt2 = me >= 2, me + 2 < total
    y_low, y_high = lax.rem(at_y + y_size - 1, y_size), lax.rem(at_y + 1, y_size)
    z_low, z_high = lax.rem(at_z + z_size - 1, z_size), lax.rem(at_z + 1, z_size)
    lines = (
        (at(at_z, y_low, at_core), at(at_z, y_high, at_core), y_size > 2, y_size > 1),
        (at(z_low, at_y, at_core), at(z_high, at_y, at_core), at_z > 0, at_z < z_size - 1),
    )
    near = [(nxt, has_nxt), (prv, has_prv), (other_core, True)]
    near += [((sp, lax.rem(tp + step, tp_size)), True) for step in range(1, tp_size)]
    for low, high, has_low, has_high in lines:
        near += [(low, has_low), (high, has_high)]
    greeted = sum(jnp.where(cond, 1, 0) for _, cond in near)

    def tell(line):
        low, high, has_low, has_high = lines[line]

        @pl.when(has_low)
        def _():
            pl.semaphore_signal(
                chain.at[2 * line + 1], inc=1, device_id=low, device_id_type=MESH
            )

        @pl.when(has_high)
        def _():
            pl.semaphore_signal(chain.at[2 * line], inc=1, device_id=high, device_id_type=MESH)

    def hear(line):
        _, _, has_low, has_high = lines[line]

        @pl.when(has_low)
        def _():
            pl.semaphore_wait(chain.at[2 * line], 1)

        @pl.when(has_high)
        def _():
            pl.semaphore_wait(chain.at[2 * line + 1], 1)

    y_rounds, z_rounds = max(y_size // 2 - 1, 0), max(z_size - 2, 0)

    def in_round(line, cond, act):
        @pl.when(cond)
        def _():
            act(line)

    barrier = pltpu.get_barrier_semaphore()
    for device, cond in near:

        @pl.when(cond)
        def _():
            pl.semaphore_signal(barrier, inc=1, device_id=device, device_id_type=MESH)

    table_load.start()
    for copy in stat_loads:
        copy.start()

    @pl.loop(0, HEADS)
    def _(k):
        for copy in loads(k):
            copy.start()

    table_load.wait()
    ext[...] = jnp.broadcast_to(table_ref[:, TABLE_LEN - 1 : TABLE_LEN], (HEADS, 512))
    ext[:, 0:TABLE_LEN] = table_ref[...]
    ext[...] = pltpu.roll(ext[...], 65, 1) * LOG2E
    key_row = lax.broadcasted_iota(jnp.int32, (HALF, HALF), 0)
    query_col = lax.broadcasted_iota(jnp.int32, (HALF, HALF), 1)
    near_off = (key_row >= SEG_LEN) & (query_col < SEG_LEN)
    far_off = (key_row < SEG_LEN) & (query_col >= SEG_LEN)

    @pl.loop(0, HEADS)
    def _(h):
        row = ext[pl.ds(h, 1), :]
        for d in range(3):
            low = row[:, HALF * d : HALF * (d + 1)]
            high = row[:, HALF * (d + 1) : HALF * (d + 2)]
            around = jnp.broadcast_to(jnp.concatenate([high, low], axis=1), (HALF, 2 * HALF))
            tile = pltpu.roll(around, 0, 1, stride=1, stride_axis=0)[:, :HALF]
            if d == 0:
                tile = jnp.where(near_off, -FAR, tile)
            bias[h, d] = tile
        flat = jnp.broadcast_to(row[:, 511:512], (HALF, HALF))
        bias[h, 3] = flat
        bias[h, 4] = jnp.where(far_off, -FAR, flat)

    pl.semaphore_wait(barrier, greeted)

    def await_loads(k):
        for copy in loads(k):
            copy.wait()

    def send_kv(k):
        @pl.when(has_nxt)
        def _():
            kv_copy(k, 0).start()

    def send_qg(k):
        @pl.when(has_prv)
        def _():
            qg_copy(HEADS - 1 - k, 0).start()

    for copy in stat_loads:
        copy.wait()

    @pl.when(has_prv)
    def _():
        st_copy(0).start()

    for k in range(2):
        await_loads(k)
        send_kv(k)
        send_qg(k)
    pl.loop(2, HEADS)(await_loads)

    def clear(buffer, start, rows):
        @pl.loop(0, HEADS)
        def _(h):
            for n in range(2):
                buffer[h, n, start : start + rows, :] = jnp.zeros((rows, HEAD_DIM), BF16)

    @pl.when(jnp.logical_not(has_prv))
    def _():
        pl.loop(2, HEADS)(send_kv)
        clear(kv, 0, 2 * ROWS)

    @pl.when(jnp.logical_not(has_nxt))
    def _():
        pl.loop(2, HEADS)(send_qg)
        clear(qg, ROWS, 2 * ROWS)
        stats[1] = jnp.zeros((2 * HEADS, ROWS), F32)
        stats[2] = jnp.zeros((2 * HEADS, ROWS), F32)

    @pl.when(me == 1)
    def _():
        clear(kv, 0, ROWS)

    @pl.when(me + 2 == total)
    def _():
        clear(qg, 2 * ROWS, ROWS)
        stats[2] = jnp.zeros((2 * HEADS, ROWS), F32)

    @pl.when(has_nxt)
    def _():
        st_copy(0).wait_recv()

        @pl.when(has_prv)
        def _():
            st_copy(1).start()

    @pl.when(has_nxt2)
    def _():
        st_copy(1).wait_recv()

    def off(cond):
        return jnp.where(cond, FAR, 0.0).astype(F32)

    key_off = [off(me < 0), off(me < 1), off(me < 2)]
    query_off = [off(me < 0), off(me + 1 >= total), off(me + 2 >= total)]
    for lag in range(3):
        for n in range(2 * HEADS):
            row = stats[lag, n : n + 1, :]
            if n < HEADS:
                row = row * LOG2E + query_off[lag]
            wide[lag, n] = jnp.broadcast_to(row, (8, ROWS))

    def tile_terms(scores, weight_grads, bias_tile, log_row, dot_row):
        weights = jnp.exp2(scores * (inv_root * LOG2E) + (bias_tile - log_row))
        return weights, weights * (weight_grads - dot_row)

    def add_to(side, part, d, score_grads):
        if part == 0:
            acc[side, d] = score_grads
        else:
            acc[side, d] += score_grads

    def query_side(h):
        for part in range(2):
            rows = pl.ds(part * HALF, HALF)
            queries, grads = qg[h, 0, rows, :], qg[h, 1, rows, :]
            keys = kv[h, 0, pl.ds(part * HALF, BAND), :]
            values = kv[h, 1, pl.ds(part * HALF, BAND), :]
            scores = dot_nt(keys, queries)
            weight_grads = dot_nt(values, grads)
            log_row = wide[0, h, 0:1, rows]
            dot_row = wide[0, HEADS + h, 0:1, rows]
            pieces = []
            for t in range(5):
                d, lag = 4 - t, 2 - (part + t) // 2
                cut = slice(t * HALF, (t + 1) * HALF)
                _, score_grads = tile_terms(
                    scores[cut], weight_grads[cut], bias[h, d], log_row + key_off[lag], dot_row
                )
                add_to(0, part, d, score_grads)
                pieces.append(score_grads.astype(BF16))
            total_grads = dot_tn(jnp.concatenate(pieces, axis=0), keys)
            dq_ref[rows, cols_of(h)] = (total_grads * inv_root).astype(BF16)

    def key_side(h):
        for part in range(2):
            rows = pl.ds(part * HALF, HALF)
            own = pl.ds(512 + part * HALF, HALF)
            keys, values = kv[h, 0, own, :], kv[h, 1, own, :]
            queries = qg[h, 0, pl.ds(part * HALF, BAND), :]
            grads = qg[h, 1, pl.ds(part * HALF, BAND), :]
            scores = dot_nt(keys, queries)
            weight_grads = dot_nt(values, grads)
            score_pieces, weight_pieces = [], []
            for d in range(5):
                lag, cols = (part + d) // 2, pl.ds((part + d) % 2 * HALF, HALF)
                cut = slice(d * HALF, (d + 1) * HALF)
                log_row = wide[lag, h, 0:1, cols]
                dot_row = wide[lag, HEADS + h, 0:1, cols]
                weights, score_grads = tile_terms(
                    scores[:, cut], weight_grads[:, cut], bias[h, d], log_row, dot_row
                )
                add_to(1, part, d, score_grads)
                score_pieces.append(score_grads.astype(BF16))
                weight_pieces.append(weights.astype(BF16))
            key_grads = dot_nn(jnp.concatenate(score_pieces, axis=1), queries)
            dk_ref[rows, cols_of(h)] = (key_grads * inv_root).astype(BF16)
            value_grads = dot_nn(jnp.concatenate(weight_pieces, axis=1), grads)
            dv_ref[rows, cols_of(h)] = value_grads.astype(BF16)

    def table_row(side, h):
        zeros = jnp.zeros((HALF, HALF), F32)
        part = jnp.concatenate([acc[side, 0], acc[side, 1], acc[side, 2], zeros], axis=1)
        for step in (64, 32, 16, 8):
            part = part[:step] + pltpu.roll(part[step:], 512 - step, 1)
        row_id = lax.broadcasted_iota(jnp.int32, (8, 512), 0)
        for step in (4, 2, 1):
            moved = pltpu.roll(part, 512 - step, 1)
            part = jnp.where((row_id & step) != 0, moved, part)
        far = jnp.sum(acc[side, 3] + acc[side, 4], keepdims=True)
        by_distance = pltpu.roll(jnp.sum(part, axis=0, keepdims=True), SEG_LEN - 1, 1)
        lane = lax.broadcasted_iota(jnp.int32, (1, 512), 1)
        top = TABLE_LEN - 1
        clipped = (lane >= top) & (lane < 448)
        far = far + jnp.sum(jnp.where(clipped, by_distance, 0.0), keepdims=True)
        row = jnp.where(lane < top, by_distance, jnp.where(lane == top, far, 0.0))
        for n in range(4):
            tab[h, n : n + 1, :] = row[:, n * HALF : (n + 1) * HALF]

    @pl.loop(0, HEADS + 1)
    def _(k):
        in_round(0, k < y_rounds, tell)
        in_round(1, 2 * k < z_rounds, tell)

        @pl.when((k < HEADS) & has_prv)
        def _():
            kv_copy(k, 0).wait_recv()

            @pl.when(has_nxt)
            def _():
                kv_copy(k, 1).start()

        @pl.when((k < HEADS) & has_nxt)
        def _():
            qg_copy(HEADS - 1 - k, 0).wait_recv()

            @pl.when(has_prv)
            def _():
                qg_copy(HEADS - 1 - k, 1).start()

        @pl.when((k < HEADS - 2) & has_prv)
        def _():
            send_kv(k + 2)

        @pl.when((k < HEADS - 2) & has_nxt)
        def _():
            send_qg(k + 2)

        in_round(1, 2 * k < z_rounds, hear)
        in_round(1, 2 * k + 1 < z_rounds, tell)

        @pl.when(k >= 1)
        def _():
            ahead, back = k - 1, HEADS - k

            @pl.when(has_prv2)
            def _():
                kv_copy(ahead, 1).wait_recv()

            query_side(ahead)

            @pl.when(k == 5)
            def _():
                over_z.start(over_y.total())

            @pl.when(k == 6)
            def _():
                over_x.start(over_z.total())

            @pl.when(k == 7)
            def _():
                over_cores.start(over_x.total())

            @pl.when(has_nxt2)
            def _():
                qg_copy(back, 1).wait_recv()

            key_side(back)

            @pl.when(k <= HEADS // 2)
            def _():
                table_row(0, ahead)
                table_row(1, back)

        in_round(0, k < y_rounds, hear)
        in_round(1, 2 * k + 1 < z_rounds, hear)

        @pl.when(k == HEADS // 2)
        def _():
            core_copy.start()
            core_copy.wait_recv()
            over_y.start(tab[pl.ds(at_core * GROUP, GROUP)] + tab_core[...])

    over_cores.receive()
    for h in range(HEADS):
        for n in range(3):
            width = min(HALF, TABLE_LEN - n * HALF)
            gt_ref[h : h + 1, n * HALF : n * HALF + width] = tab_all[
                h // GROUP, h % GROUP, n : n + 1, :width
            ]

    @pl.when(has_nxt)
    def _():
        @pl.loop(0, HEADS)
        def _(h):
            kv_copy(h, 0).wait_send()

            @pl.when(has_prv)
            def _():
                kv_copy(h, 1).wait_send()

    @pl.when(has_prv)
    def _():
        st_copy(0).wait_send()

        @pl.when(has_nxt)
        def _():
            st_copy(1).wait_send()

        @pl.loop(0, HEADS)
        def _(h):
            qg_copy(h, 0).wait_send()

            @pl.when(has_nxt)
            def _():
                qg_copy(h, 1).wait_send()

    core_copy.wait_send()
    for line in (over_y, over_z, over_x, over_cores):
        line.finish()


def write_out(*refs):
    count = len(refs) // 2
    copies = [
        pltpu.make_async_copy(refs[n], refs[count + n], refs[-1].at[n]) for n in range(count)
    ]
    for copy in copies:
        copy.start()
    for copy in copies:
        copy.wait()


def solution(mesh):
    sp_size, tp_size = mesh.shape["sp"], mesh.shape["tp"]

    def local(query_rows, key_rows, value_rows, out_grad, log_totals, out_dot, bias_table):
        hbm = pl.BlockSpec(memory_space=pltpu.HBM)
        z_size, y_size, core_size = SP_SHAPE
        tiles = (GROUP, 4, HALF)

        def in_hbm(array):
            return pltpu.with_memory_space_constraint(array, pltpu.HBM)

        vmem = pl.BlockSpec(memory_space=pltpu.VMEM)
        rows = jax.ShapeDtypeStruct(query_rows.shape, BF16)
        shapes = (rows, rows, rows, jax.ShapeDtypeStruct(bias_table.shape, F32))
        results = pl.pallas_call(
            functools.partial(kernel, sp_size, tp_size),
            out_shape=shapes,
            in_specs=[hbm] * 7,
            out_specs=(vmem, vmem, vmem, vmem),
            scratch_shapes=[
                pltpu.VMEM((HEADS, 2, 3 * ROWS, HEAD_DIM), BF16),
                pltpu.VMEM((HEADS, 2, 3 * ROWS, HEAD_DIM), BF16),
                pltpu.VMEM((3, 2 * HEADS, ROWS), F32),
                pltpu.VMEM((3, 2 * HEADS, 8, ROWS), F32),
                pltpu.VMEM((HEADS, 5, HALF, HALF), F32),
                pltpu.VMEM((HEADS, TABLE_LEN), F32),
                pltpu.VMEM((HEADS, 512), F32),
                pltpu.VMEM((2, 5, HALF, HALF), F32),
                pltpu.VMEM((HEADS, 4, HALF), F32),
                pltpu.VMEM(tiles, F32),
                pltpu.VMEM((y_size,) + tiles, F32),
                pltpu.VMEM((z_size,) + tiles, F32),
                pltpu.VMEM((tp_size,) + tiles, F32),
                pltpu.VMEM((core_size,) + tiles, F32),
                pltpu.SemaphoreType.DMA((4, HEADS)),
                pltpu.SemaphoreType.DMA((3,)),
                pltpu.SemaphoreType.REGULAR((4,)),
                pltpu.SemaphoreType.DMA((2,)),
                pltpu.SemaphoreType.DMA((y_size,)),
                pltpu.SemaphoreType.DMA((y_size,)),
                pltpu.SemaphoreType.DMA((z_size,)),
                pltpu.SemaphoreType.DMA((z_size,)),
                pltpu.SemaphoreType.DMA((tp_size,)),
                pltpu.SemaphoreType.DMA((tp_size,)),
                pltpu.SemaphoreType.DMA((core_size,)),
                pltpu.SemaphoreType.DMA((core_size,)),
                pltpu.SemaphoreType.DMA((2, HEADS)),
                pltpu.SemaphoreType.DMA((2, HEADS)),
                pltpu.SemaphoreType.DMA((2, HEADS)),
                pltpu.SemaphoreType.DMA((2, HEADS)),
                pltpu.SemaphoreType.DMA((2,)),
                pltpu.SemaphoreType.DMA((2,)),
            ],
            compiler_params=pltpu.CompilerParams(
                collective_id=0, has_side_effects=True, vmem_limit_bytes=32 * 2**20
            ),
        )(*map(in_hbm, (query_rows, key_rows, value_rows, out_grad, log_totals.T, out_dot.T, bias_table)))
        return pl.pallas_call(
            write_out,
            out_shape=shapes,
            in_specs=[vmem] * 4,
            out_specs=(hbm,) * 4,
            scratch_shapes=[pltpu.SemaphoreType.DMA((4,))],
        )(*(pltpu.with_memory_space_constraint(part, pltpu.VMEM) for part in results))

    split = P(("sp", "tp"), None)
    return jax.shard_map(
        local,
        mesh=mesh,
        in_specs=(split,) * 6 + (P(),),
        out_specs=(split, split, split, P()),
        check_vma=False,
    )
```

```python
import functools
import math

import jax
import jax.numpy as jnp
from jax import lax
from jax.experimental import pallas as pl
from jax.experimental.pallas import tpu as pltpu
from jax.sharding import PartitionSpec as P

SEG_LEN = 64
REL_CLIP = 256
ROWS = 256
HALF = 128
BAND = 640
HEADS = 8
HEAD_DIM = 128
TABLE_LEN = 320
LOG2E = math.log2(math.e)
FAR = 1e30
SP_SHAPE = (12, 8, 2)
GROUP = HEADS // 2
MESH = pl.DeviceIdType.MESH
F32 = jnp.float32
BF16 = jnp.bfloat16


def dot_nt(lhs, rhs):
    return lax.dot_general(lhs, rhs, (((1,), (1,)), ((), ())), preferred_element_type=F32)


def dot_nn(lhs, rhs):
    return lax.dot_general(lhs, rhs, (((1,), (0,)), ((), ())), preferred_element_type=F32)


def dot_tn(lhs, rhs):
    return lax.dot_general(lhs, rhs, (((0,), (0,)), ((), ())), preferred_element_type=F32)


def kernel(
    sp_size,
    tp_size,
    q_hbm,
    k_hbm,
    v_hbm,
    g_hbm,
    lse_hbm,
    dot_hbm,
    table_hbm,
    dq_ref,
    dk_ref,
    dv_ref,
    gt_ref,
    kv,
    qg,
    stats,
    wide,
    bias,
    table_ref,
    ext,
    acc,
    tab,
    tab_core,
    tab_y,
    tab_z,
    tab_x,
    tab_all,
    load_sem,
    stat_sem,
    chain,
    core_sem,
    y_send,
    y_recv,
    z_send,
    z_recv,
    x_send,
    x_recv,
    all_send,
    all_recv,
    kv_send,
    kv_recv,
    qg_send,
    qg_recv,
    st_send,
    st_recv,
):
    sp, tp = lax.axis_index("sp"), lax.axis_index("tp")
    last_tp, first_tp = tp == tp_size - 1, tp == 0
    nxt = (
        lax.rem(sp + jnp.where(last_tp, 1, 0), sp_size),
        lax.rem(tp + 1, tp_size),
    )
    prv = (
        lax.rem(sp + sp_size - jnp.where(first_tp, 1, 0), sp_size),
        lax.rem(tp + tp_size - 1, tp_size),
    )
    z_size, y_size, core_size = SP_SHAPE
    at_z, at_y, at_core = sp // (y_size * core_size), sp // core_size % y_size, sp % core_size

    def at(z, y, core):
        return ((z * y_size + y) * core_size + core, tp)

    me = sp * tp_size + tp
    total = sp_size * tp_size
    inv_root = HEAD_DIM**-0.5

    def cols_of(h):
        return pl.ds(pl.multiple_of(h * HEAD_DIM, HEAD_DIM), HEAD_DIM)

    def loads(k):
        ahead, back = k, HEADS - 1 - k
        places = [
            (k_hbm, kv.at[ahead, 0, pl.ds(512, ROWS)], ahead),
            (v_hbm, kv.at[ahead, 1, pl.ds(512, ROWS)], ahead),
            (q_hbm, qg.at[back, 0, pl.ds(0, ROWS)], back),
            (g_hbm, qg.at[back, 1, pl.ds(0, ROWS)], back),
        ]
        return [
            pltpu.make_async_copy(
                src.at[:, cols_of(h)],
                dst,
                load_sem.at[n, h],
            )
            for n, (src, dst, h) in enumerate(places)
        ]

    def kv_copy(h, lag):
        src, dst = (512, 256) if lag == 0 else (256, 0)
        return pltpu.make_async_remote_copy(
            src_ref=kv.at[h, :, pl.ds(src, ROWS)],
            dst_ref=kv.at[h, :, pl.ds(dst, ROWS)],
            send_sem=kv_send.at[lag, h],
            recv_sem=kv_recv.at[lag, h],
            device_id=nxt,
            device_id_type=MESH,
        )

    def qg_copy(h, lag):
        return pltpu.make_async_remote_copy(
            src_ref=qg.at[h, :, pl.ds(lag * ROWS, ROWS)],
            dst_ref=qg.at[h, :, pl.ds((lag + 1) * ROWS, ROWS)],
            send_sem=qg_send.at[lag, h],
            recv_sem=qg_recv.at[lag, h],
            device_id=prv,
            device_id_type=MESH,
        )

    def st_copy(lag):
        return pltpu.make_async_remote_copy(
            src_ref=stats.at[lag],
            dst_ref=stats.at[lag + 1],
            send_sem=st_send.at[lag],
            recv_sem=st_recv.at[lag],
            device_id=prv,
            device_id_type=MESH,
        )

    class Exchange:
        def __init__(self, slots, size, mine, device, send, recv):
            self.slots, self.size, self.mine = slots, size, mine
            self.device, self.send, self.recv = device, send, recv

        def other(self, step):
            return lax.rem(self.mine + step, self.size)

        def copy(self, step, slot):
            return pltpu.make_async_remote_copy(
                src_ref=self.slots.at[slot],
                dst_ref=self.slots.at[slot],
                send_sem=self.send.at[step],
                recv_sem=self.recv.at[slot],
                device_id=self.device(self.other(step)),
                device_id_type=MESH,
            )

        def start(self, value):
            self.slots[self.mine] = value

            @pl.loop(1, self.size)
            def _(step):
                self.copy(step, self.mine).start()

        def receive(self):
            @pl.loop(1, self.size)
            def _(step):
                self.copy(step, self.other(step)).wait_recv()

        def total(self):
            self.receive()
            value = self.slots[0]
            for slot in range(1, self.size):
                value = value + self.slots[slot]
            return value

        def finish(self):
            @pl.loop(1, self.size)
            def _(step):
                self.copy(step, self.mine).wait_send()

    over_y = Exchange(tab_y, y_size, at_y, lambda y: at(at_z, y, at_core), y_send, y_recv)
    over_z = Exchange(tab_z, z_size, at_z, lambda z: at(z, at_y, at_core), z_send, z_recv)
    over_x = Exchange(tab_x, tp_size, tp, lambda x: (sp, x), x_send, x_recv)
    other_core = at(at_z, at_y, 1 - at_core)
    over_cores = Exchange(
        tab_all, core_size, at_core, lambda core: at(at_z, at_y, core), all_send, all_recv
    )
    core_copy = pltpu.make_async_remote_copy(
        src_ref=tab.at[pl.ds((1 - at_core) * GROUP, GROUP)],
        dst_ref=tab_core,
        send_sem=core_sem.at[0],
        recv_sem=core_sem.at[1],
        device_id=other_core,
        device_id_type=MESH,
    )

    stat_loads = [
        pltpu.make_async_copy(lse_hbm, stats.at[0, pl.ds(0, HEADS)], stat_sem.at[0]),
        pltpu.make_async_copy(dot_hbm, stats.at[0, pl.ds(HEADS, HEADS)], stat_sem.at[1]),
    ]
    table_load = pltpu.make_async_copy(table_hbm, table_ref, stat_sem.at[2])

    has_prv, has_nxt = me >= 1, me + 1 < total
    has_prv2, has_nxt2 = me >= 2, me + 2 < total
    y_low, y_high = lax.rem(at_y + y_size - 1, y_size), lax.rem(at_y + 1, y_size)
    z_low, z_high = lax.rem(at_z + z_size - 1, z_size), lax.rem(at_z + 1, z_size)
    lines = (
        (at(at_z, y_low, at_core), at(at_z, y_high, at_core), y_size > 2, y_size > 1),
        (at(z_low, at_y, at_core), at(z_high, at_y, at_core), at_z > 0, at_z < z_size - 1),
    )
    near = [(nxt, has_nxt), (prv, has_prv), (other_core, True)]
    near += [((sp, lax.rem(tp + step, tp_size)), True) for step in range(1, tp_size)]
    for low, high, has_low, has_high in lines:
        near += [(low, has_low), (high, has_high)]
    greeted = sum(jnp.where(cond, 1, 0) for _, cond in near)

    def tell(line):
        low, high, has_low, has_high = lines[line]

        @pl.when(has_low)
        def _():
            pl.semaphore_signal(
                chain.at[2 * line + 1], inc=1, device_id=low, device_id_type=MESH
            )

        @pl.when(has_high)
        def _():
            pl.semaphore_signal(chain.at[2 * line], inc=1, device_id=high, device_id_type=MESH)

    def hear(line):
        _, _, has_low, has_high = lines[line]

        @pl.when(has_low)
        def _():
            pl.semaphore_wait(chain.at[2 * line], 1)

        @pl.when(has_high)
        def _():
            pl.semaphore_wait(chain.at[2 * line + 1], 1)

    y_rounds, z_rounds = max(y_size // 2 - 1, 0), max(z_size - 2, 0)

    def in_round(line, cond, act):
        @pl.when(cond)
        def _():
            act(line)

    barrier = pltpu.get_barrier_semaphore()
    for device, cond in near:

        @pl.when(cond)
        def _():
            pl.semaphore_signal(barrier, inc=1, device_id=device, device_id_type=MESH)

    table_load.start()
    for copy in stat_loads:
        copy.start()

    @pl.loop(0, HEADS)
    def _(k):
        for copy in loads(k):
            copy.start()

    table_load.wait()
    ext[...] = jnp.broadcast_to(table_ref[:, TABLE_LEN - 1 : TABLE_LEN], (HEADS, 512))
    ext[:, 0:TABLE_LEN] = table_ref[...]
    ext[...] = pltpu.roll(ext[...], 65, 1) * LOG2E
    key_row = lax.broadcasted_iota(jnp.int32, (HALF, HALF), 0)
    query_col = lax.broadcasted_iota(jnp.int32, (HALF, HALF), 1)
    near_off = (key_row >= SEG_LEN) & (query_col < SEG_LEN)
    far_off = (key_row < SEG_LEN) & (query_col >= SEG_LEN)

    @pl.loop(0, HEADS)
    def _(h):
        row = ext[pl.ds(h, 1), :]
        for d in range(3):
            low = row[:, HALF * d : HALF * (d + 1)]
            high = row[:, HALF * (d + 1) : HALF * (d + 2)]
            around = jnp.broadcast_to(jnp.concatenate([high, low], axis=1), (HALF, 2 * HALF))
            tile = pltpu.roll(around, 0, 1, stride=1, stride_axis=0)[:, :HALF]
            if d == 0:
                tile = jnp.where(near_off, -FAR, tile)
            bias[h, d] = tile
        flat = jnp.broadcast_to(row[:, 511:512], (HALF, HALF))
        bias[h, 3] = flat
        bias[h, 4] = jnp.where(far_off, -FAR, flat)

    pl.semaphore_wait(barrier, greeted)

    def await_loads(k):
        for copy in loads(k):
            copy.wait()

    def send_kv(k):
        @pl.when(has_nxt)
        def _():
            kv_copy(k, 0).start()

    def send_qg(k):
        @pl.when(has_prv)
        def _():
            qg_copy(HEADS - 1 - k, 0).start()

    for copy in stat_loads:
        copy.wait()

    @pl.when(has_prv)
    def _():
        st_copy(0).start()

    for k in range(2):
        await_loads(k)
        send_kv(k)
        send_qg(k)
    pl.loop(2, HEADS)(await_loads)

    def clear(buffer, start, rows):
        @pl.loop(0, HEADS)
        def _(h):
            for n in range(2):
                buffer[h, n, start : start + rows, :] = jnp.zeros((rows, HEAD_DIM), BF16)

    @pl.when(jnp.logical_not(has_prv))
    def _():
        pl.loop(2, HEADS)(send_kv)
        clear(kv, 0, 2 * ROWS)

    @pl.when(jnp.logical_not(has_nxt))
    def _():
        pl.loop(2, HEADS)(send_qg)
        clear(qg, ROWS, 2 * ROWS)
        stats[1] = jnp.zeros((2 * HEADS, ROWS), F32)
        stats[2] = jnp.zeros((2 * HEADS, ROWS), F32)

    @pl.when(me == 1)
    def _():
        clear(kv, 0, ROWS)

    @pl.when(me + 2 == total)
    def _():
        clear(qg, 2 * ROWS, ROWS)
        stats[2] = jnp.zeros((2 * HEADS, ROWS), F32)

    @pl.when(has_nxt)
    def _():
        st_copy(0).wait_recv()

        @pl.when(has_prv)
        def _():
            st_copy(1).start()

    @pl.when(has_nxt2)
    def _():
        st_copy(1).wait_recv()

    def off(cond):
        return jnp.where(cond, FAR, 0.0).astype(F32)

    key_off = [off(me < 0), off(me < 1), off(me < 2)]
    query_off = [off(me < 0), off(me + 1 >= total), off(me + 2 >= total)]
    for lag in range(3):
        for n in range(2 * HEADS):
            row = stats[lag, n : n + 1, :]
            if n < HEADS:
                row = row * LOG2E + query_off[lag]
            wide[lag, n] = jnp.broadcast_to(row, (8, ROWS))

    def tile_terms(scores, weight_grads, bias_tile, log_row, dot_row):
        weights = jnp.exp2(scores * (inv_root * LOG2E) + (bias_tile - log_row))
        return weights, weights * (weight_grads - dot_row)

    def add_to(side, part, d, score_grads):
        if part == 0:
            acc[side, d] = score_grads
        else:
            acc[side, d] += score_grads

    def query_side(h):
        for part in range(2):
            rows = pl.ds(part * HALF, HALF)
            queries, grads = qg[h, 0, rows, :], qg[h, 1, rows, :]
            keys = kv[h, 0, pl.ds(part * HALF, BAND), :]
            values = kv[h, 1, pl.ds(part * HALF, BAND), :]
            scores = dot_nt(keys, queries)
            weight_grads = dot_nt(values, grads)
            log_row = wide[0, h, 0:1, rows]
            dot_row = wide[0, HEADS + h, 0:1, rows]
            pieces = []
            for t in range(5):
                d, lag = 4 - t, 2 - (part + t) // 2
                cut = slice(t * HALF, (t + 1) * HALF)
                _, score_grads = tile_terms(
                    scores[cut], weight_grads[cut], bias[h, d], log_row + key_off[lag], dot_row
                )
                add_to(0, part, d, score_grads)
                pieces.append(score_grads.astype(BF16))
            total_grads = dot_tn(jnp.concatenate(pieces, axis=0), keys)
            dq_ref[rows, cols_of(h)] = (total_grads * inv_root).astype(BF16)

    def key_side(h):
        for part in range(2):
            rows = pl.ds(part * HALF, HALF)
            own = pl.ds(512 + part * HALF, HALF)
            keys, values = kv[h, 0, own, :], kv[h, 1, own, :]
            queries = qg[h, 0, pl.ds(part * HALF, BAND), :]
            grads = qg[h, 1, pl.ds(part * HALF, BAND), :]
            scores = dot_nt(keys, queries)
            weight_grads = dot_nt(values, grads)
            score_pieces, weight_pieces = [], []
            for d in range(5):
                lag, cols = (part + d) // 2, pl.ds((part + d) % 2 * HALF, HALF)
                cut = slice(d * HALF, (d + 1) * HALF)
                log_row = wide[lag, h, 0:1, cols]
                dot_row = wide[lag, HEADS + h, 0:1, cols]
                weights, score_grads = tile_terms(
                    scores[:, cut], weight_grads[:, cut], bias[h, d], log_row, dot_row
                )
                add_to(1, part, d, score_grads)
                score_pieces.append(score_grads.astype(BF16))
                weight_pieces.append(weights.astype(BF16))
            key_grads = dot_nn(jnp.concatenate(score_pieces, axis=1), queries)
            dk_ref[rows, cols_of(h)] = (key_grads * inv_root).astype(BF16)
            value_grads = dot_nn(jnp.concatenate(weight_pieces, axis=1), grads)
            dv_ref[rows, cols_of(h)] = value_grads.astype(BF16)

    def table_row(side, h):
        zeros = jnp.zeros((HALF, HALF), F32)
        part = jnp.concatenate([acc[side, 0], acc[side, 1], acc[side, 2], zeros], axis=1)
        for step in (64, 32, 16, 8):
            part = part[:step] + pltpu.roll(part[step:], 512 - step, 1)
        row_id = lax.broadcasted_iota(jnp.int32, (8, 512), 0)
        for step in (4, 2, 1):
            moved = pltpu.roll(part, 512 - step, 1)
            part = jnp.where((row_id & step) != 0, moved, part)
        far = jnp.sum(acc[side, 3] + acc[side, 4], keepdims=True)
        by_distance = pltpu.roll(jnp.sum(part, axis=0, keepdims=True), SEG_LEN - 1, 1)
        lane = lax.broadcasted_iota(jnp.int32, (1, 512), 1)
        top = TABLE_LEN - 1
        clipped = (lane >= top) & (lane < 448)
        far = far + jnp.sum(jnp.where(clipped, by_distance, 0.0), keepdims=True)
        row = jnp.where(lane < top, by_distance, jnp.where(lane == top, far, 0.0))
        for n in range(4):
            tab[h, n : n + 1, :] = row[:, n * HALF : (n + 1) * HALF]

    def forward(k):
        @pl.when(has_prv)
        def _():
            kv_copy(k, 0).wait_recv()

            @pl.when(has_nxt)
            def _():
                kv_copy(k, 1).start()

        @pl.when(has_nxt)
        def _():
            qg_copy(HEADS - 1 - k, 0).wait_recv()

            @pl.when(has_prv)
            def _():
                qg_copy(HEADS - 1 - k, 1).start()

    def send_own(k):
        @pl.when(has_prv)
        def _():
            send_kv(k)

        @pl.when(has_nxt)
        def _():
            send_qg(k)

    @pl.loop(0, HEADS + 1)
    def _(k):
        in_round(0, k < y_rounds, tell)
        in_round(1, 2 * k < z_rounds, tell)

        @pl.when(k < GROUP)
        def _():
            forward(k)

        @pl.when(k < 2)
        def _():
            send_own(k + 2)

        @pl.when(k == 3)
        def _():
            send_own(4)

        in_round(1, 2 * k < z_rounds, hear)
        in_round(1, 2 * k + 1 < z_rounds, tell)

        @pl.when(k >= 1)
        def _():
            ahead, back = k - 1, HEADS - k

            @pl.when(has_prv2)
            def _():
                kv_copy(ahead, 1).wait_recv()

            query_side(ahead)

            @pl.when(k == HEADS)
            def _():
                over_cores.start(over_z.total())

            @pl.when(has_nxt2)
            def _():
                qg_copy(back, 1).wait_recv()

            key_side(back)

            @pl.when(k <= GROUP)
            def _():
                table_row(0, ahead)
                table_row(1, back)

        in_round(0, k < y_rounds, hear)
        in_round(1, 2 * k + 1 < z_rounds, hear)

        @pl.when(k == GROUP)
        def _():
            over_x.start(tab[...])
            pl.loop(5, HEADS)(send_own)
            forward(4)
            tab[...] = over_x.total()
            core_copy.start()
            core_copy.wait_recv()
            over_y.start(tab[pl.ds(at_core * GROUP, GROUP)] + tab_core[...])
            pl.loop(5, HEADS)(forward)
            over_z.start(over_y.total())

    over_cores.receive()
    for h in range(HEADS):
        for n in range(3):
            width = min(HALF, TABLE_LEN - n * HALF)
            gt_ref[h : h + 1, n * HALF : n * HALF + width] = tab_all[
                h // GROUP, h % GROUP, n : n + 1, :width
            ]

    @pl.when(has_nxt)
    def _():
        @pl.loop(0, HEADS)
        def _(h):
            kv_copy(h, 0).wait_send()

            @pl.when(has_prv)
            def _():
                kv_copy(h, 1).wait_send()

    @pl.when(has_prv)
    def _():
        st_copy(0).wait_send()

        @pl.when(has_nxt)
        def _():
            st_copy(1).wait_send()

        @pl.loop(0, HEADS)
        def _(h):
            qg_copy(h, 0).wait_send()

            @pl.when(has_nxt)
            def _():
                qg_copy(h, 1).wait_send()

    core_copy.wait_send()
    for line in (over_y, over_z, over_x, over_cores):
        line.finish()


def write_out(*refs):
    count = len(refs) // 2
    copies = [
        pltpu.make_async_copy(refs[n], refs[count + n], refs[-1].at[n]) for n in range(count)
    ]
    for copy in copies:
        copy.start()
    for copy in copies:
        copy.wait()


def solution(mesh):
    sp_size, tp_size = mesh.shape["sp"], mesh.shape["tp"]

    def local(query_rows, key_rows, value_rows, out_grad, log_totals, out_dot, bias_table):
        hbm = pl.BlockSpec(memory_space=pltpu.HBM)
        z_size, y_size, core_size = SP_SHAPE
        tiles = (GROUP, 4, HALF)

        def in_hbm(array):
            return pltpu.with_memory_space_constraint(array, pltpu.HBM)

        vmem = pl.BlockSpec(memory_space=pltpu.VMEM)
        rows = jax.ShapeDtypeStruct(query_rows.shape, BF16)
        shapes = (rows, rows, rows, jax.ShapeDtypeStruct(bias_table.shape, F32))
        results = pl.pallas_call(
            functools.partial(kernel, sp_size, tp_size),
            out_shape=shapes,
            in_specs=[hbm] * 7,
            out_specs=(vmem, vmem, vmem, vmem),
            scratch_shapes=[
                pltpu.VMEM((HEADS, 2, 3 * ROWS, HEAD_DIM), BF16),
                pltpu.VMEM((HEADS, 2, 3 * ROWS, HEAD_DIM), BF16),
                pltpu.VMEM((3, 2 * HEADS, ROWS), F32),
                pltpu.VMEM((3, 2 * HEADS, 8, ROWS), F32),
                pltpu.VMEM((HEADS, 5, HALF, HALF), F32),
                pltpu.VMEM((HEADS, TABLE_LEN), F32),
                pltpu.VMEM((HEADS, 512), F32),
                pltpu.VMEM((2, 5, HALF, HALF), F32),
                pltpu.VMEM((HEADS, 4, HALF), F32),
                pltpu.VMEM(tiles, F32),
                pltpu.VMEM((y_size,) + tiles, F32),
                pltpu.VMEM((z_size,) + tiles, F32),
                pltpu.VMEM((tp_size, HEADS) + tiles[1:], F32),
                pltpu.VMEM((core_size,) + tiles, F32),
                pltpu.SemaphoreType.DMA((4, HEADS)),
                pltpu.SemaphoreType.DMA((3,)),
                pltpu.SemaphoreType.REGULAR((4,)),
                pltpu.SemaphoreType.DMA((2,)),
                pltpu.SemaphoreType.DMA((y_size,)),
                pltpu.SemaphoreType.DMA((y_size,)),
                pltpu.SemaphoreType.DMA((z_size,)),
                pltpu.SemaphoreType.DMA((z_size,)),
                pltpu.SemaphoreType.DMA((tp_size,)),
                pltpu.SemaphoreType.DMA((tp_size,)),
                pltpu.SemaphoreType.DMA((core_size,)),
                pltpu.SemaphoreType.DMA((core_size,)),
                pltpu.SemaphoreType.DMA((2, HEADS)),
                pltpu.SemaphoreType.DMA((2, HEADS)),
                pltpu.SemaphoreType.DMA((2, HEADS)),
                pltpu.SemaphoreType.DMA((2, HEADS)),
                pltpu.SemaphoreType.DMA((2,)),
                pltpu.SemaphoreType.DMA((2,)),
            ],
            compiler_params=pltpu.CompilerParams(
                collective_id=0, has_side_effects=True, vmem_limit_bytes=32 * 2**20
            ),
        )(*map(in_hbm, (query_rows, key_rows, value_rows, out_grad, log_totals.T, out_dot.T, bias_table)))
        return pl.pallas_call(
            write_out,
            out_shape=shapes,
            in_specs=[vmem] * 4,
            out_specs=(hbm,) * 4,
            scratch_shapes=[pltpu.SemaphoreType.DMA((4,))],
        )(*(pltpu.with_memory_space_constraint(part, pltpu.VMEM) for part in results))

    split = P(("sp", "tp"), None)
    return jax.shard_map(
        local,
        mesh=mesh,
        in_specs=(split,) * 6 + (P(),),
        out_specs=(split, split, split, P()),
        check_vma=False,
    )
```

```python
import functools
import math

import jax
import jax.numpy as jnp
from jax import lax
from jax.experimental import pallas as pl
from jax.experimental.pallas import tpu as pltpu
from jax.sharding import PartitionSpec as P

SEG_LEN = 64
REL_CLIP = 256
ROWS = 256
HALF = 128
BAND = 640
HEADS = 8
HEAD_DIM = 128
TABLE_LEN = 320
LOG2E = math.log2(math.e)
FAR = 1e30
SP_SHAPE = (12, 8, 2)
GROUP = HEADS // 2
MESH = pl.DeviceIdType.MESH
F32 = jnp.float32
BF16 = jnp.bfloat16


def dot_nt(lhs, rhs):
    return lax.dot_general(lhs, rhs, (((1,), (1,)), ((), ())), preferred_element_type=F32)


def dot_nn(lhs, rhs):
    return lax.dot_general(lhs, rhs, (((1,), (0,)), ((), ())), preferred_element_type=F32)


def dot_tn(lhs, rhs):
    return lax.dot_general(lhs, rhs, (((0,), (0,)), ((), ())), preferred_element_type=F32)


def kernel(
    sp_size,
    tp_size,
    q_hbm,
    k_hbm,
    v_hbm,
    g_hbm,
    lse_hbm,
    dot_hbm,
    table_hbm,
    dq_ref,
    dk_ref,
    dv_ref,
    gt_ref,
    kv,
    qg,
    stats,
    wide,
    bias,
    table_ref,
    ext,
    acc,
    tab,
    tab_half,
    tab_core,
    tab_y,
    tab_z,
    tab_row,
    load_sem,
    stat_sem,
    chain,
    core_sem,
    y_send,
    y_recv,
    z_send,
    z_recv,
    row_send,
    row_recv,
    kv_send,
    kv_recv,
    qg_send,
    qg_recv,
    st_send,
    st_recv,
):
    sp, tp = lax.axis_index("sp"), lax.axis_index("tp")
    last_tp, first_tp = tp == tp_size - 1, tp == 0
    nxt = (
        lax.rem(sp + jnp.where(last_tp, 1, 0), sp_size),
        lax.rem(tp + 1, tp_size),
    )
    prv = (
        lax.rem(sp + sp_size - jnp.where(first_tp, 1, 0), sp_size),
        lax.rem(tp + tp_size - 1, tp_size),
    )
    z_size, y_size, core_size = SP_SHAPE
    at_z, at_y, at_core = sp // (y_size * core_size), sp // core_size % y_size, sp % core_size

    def at(z, y, core):
        return ((z * y_size + y) * core_size + core, tp)

    me = sp * tp_size + tp
    total = sp_size * tp_size
    inv_root = HEAD_DIM**-0.5

    def cols_of(h):
        return pl.ds(pl.multiple_of(h * HEAD_DIM, HEAD_DIM), HEAD_DIM)

    def loads(k):
        ahead, back = k, HEADS - 1 - k
        places = [
            (k_hbm, kv.at[ahead, 0, pl.ds(512, ROWS)], ahead),
            (v_hbm, kv.at[ahead, 1, pl.ds(512, ROWS)], ahead),
            (q_hbm, qg.at[back, 0, pl.ds(0, ROWS)], back),
            (g_hbm, qg.at[back, 1, pl.ds(0, ROWS)], back),
        ]
        return [
            pltpu.make_async_copy(
                src.at[:, cols_of(h)],
                dst,
                load_sem.at[n, h],
            )
            for n, (src, dst, h) in enumerate(places)
        ]

    def kv_copy(h, lag):
        src, dst = (512, 256) if lag == 0 else (256, 0)
        return pltpu.make_async_remote_copy(
            src_ref=kv.at[h, :, pl.ds(src, ROWS)],
            dst_ref=kv.at[h, :, pl.ds(dst, ROWS)],
            send_sem=kv_send.at[lag, h],
            recv_sem=kv_recv.at[lag, h],
            device_id=nxt,
            device_id_type=MESH,
        )

    def qg_copy(h, lag):
        return pltpu.make_async_remote_copy(
            src_ref=qg.at[h, :, pl.ds(lag * ROWS, ROWS)],
            dst_ref=qg.at[h, :, pl.ds((lag + 1) * ROWS, ROWS)],
            send_sem=qg_send.at[lag, h],
            recv_sem=qg_recv.at[lag, h],
            device_id=prv,
            device_id_type=MESH,
        )

    def st_copy(lag):
        return pltpu.make_async_remote_copy(
            src_ref=stats.at[lag],
            dst_ref=stats.at[lag + 1],
            send_sem=st_send.at[lag],
            recv_sem=st_recv.at[lag],
            device_id=prv,
            device_id_type=MESH,
        )

    class Exchange:
        def __init__(self, slots, size, mine, device, send, recv):
            self.slots, self.size, self.mine = slots, size, mine
            self.device, self.send, self.recv = device, send, recv

        def other(self, step):
            return lax.rem(self.mine + step, self.size)

        def copy(self, step, slot):
            return pltpu.make_async_remote_copy(
                src_ref=self.slots.at[slot],
                dst_ref=self.slots.at[slot],
                send_sem=self.send.at[step],
                recv_sem=self.recv.at[slot],
                device_id=self.device(self.other(step)),
                device_id_type=MESH,
            )

        def start(self, value):
            self.slots[self.mine] = value

            @pl.loop(1, self.size)
            def _(step):
                self.copy(step, self.mine).start()

        def receive(self):
            @pl.loop(1, self.size)
            def _(step):
                self.copy(step, self.other(step)).wait_recv()

        def total(self):
            self.receive()
            value = self.slots[0]
            for slot in range(1, self.size):
                value = value + self.slots[slot]
            return value

        def finish(self):
            @pl.loop(1, self.size)
            def _(step):
                self.copy(step, self.mine).wait_send()

    over_y = Exchange(tab_y, y_size, at_y, lambda y: at(at_z, y, at_core), y_send, y_recv)
    over_z = Exchange(tab_z, z_size, at_z, lambda z: at(z, at_y, at_core), z_send, z_recv)
    row_size = core_size * tp_size
    over_row = Exchange(
        tab_row,
        row_size,
        at_core * tp_size + tp,
        lambda e: (at(at_z, at_y, e // tp_size)[0], lax.rem(e, tp_size)),
        row_send,
        row_recv,
    )
    other_core = at(at_z, at_y, 1 - at_core)
    core_copy = pltpu.make_async_remote_copy(
        src_ref=tab_half.at[1 - at_core],
        dst_ref=tab_core,
        send_sem=core_sem.at[0],
        recv_sem=core_sem.at[1],
        device_id=other_core,
        device_id_type=MESH,
    )

    stat_loads = [
        pltpu.make_async_copy(lse_hbm, stats.at[0, pl.ds(0, HEADS)], stat_sem.at[0]),
        pltpu.make_async_copy(dot_hbm, stats.at[0, pl.ds(HEADS, HEADS)], stat_sem.at[1]),
    ]
    table_load = pltpu.make_async_copy(table_hbm, table_ref, stat_sem.at[2])

    has_prv, has_nxt = me >= 1, me + 1 < total
    has_prv2, has_nxt2 = me >= 2, me + 2 < total
    y_low, y_high = lax.rem(at_y + y_size - 1, y_size), lax.rem(at_y + 1, y_size)
    z_low, z_high = lax.rem(at_z + z_size - 1, z_size), lax.rem(at_z + 1, z_size)
    lines = (
        (at(at_z, y_low, at_core), at(at_z, y_high, at_core), y_size > 2, y_size > 1),
        (at(z_low, at_y, at_core), at(z_high, at_y, at_core), at_z > 0, at_z < z_size - 1),
    )
    near = [(nxt, has_nxt), (prv, has_prv)]
    near += [(over_row.device(over_row.other(step)), True) for step in range(1, row_size)]
    for low, high, has_low, has_high in lines:
        near += [(low, has_low), (high, has_high)]
    greeted = sum(jnp.where(cond, 1, 0) for _, cond in near)

    def tell(line):
        low, high, has_low, has_high = lines[line]

        @pl.when(has_low)
        def _():
            pl.semaphore_signal(
                chain.at[2 * line + 1], inc=1, device_id=low, device_id_type=MESH
            )

        @pl.when(has_high)
        def _():
            pl.semaphore_signal(chain.at[2 * line], inc=1, device_id=high, device_id_type=MESH)

    def hear(line):
        _, _, has_low, has_high = lines[line]

        @pl.when(has_low)
        def _():
            pl.semaphore_wait(chain.at[2 * line], 1)

        @pl.when(has_high)
        def _():
            pl.semaphore_wait(chain.at[2 * line + 1], 1)

    y_rounds, z_rounds = max(y_size // 2 - 1, 0), max(z_size - 2, 0)

    def in_round(line, cond, act):
        @pl.when(cond)
        def _():
            act(line)

    barrier = pltpu.get_barrier_semaphore()
    for device, cond in near:

        @pl.when(cond)
        def _():
            pl.semaphore_signal(barrier, inc=1, device_id=device, device_id_type=MESH)

    table_load.start()
    for copy in stat_loads:
        copy.start()

    @pl.loop(0, HEADS)
    def _(k):
        for copy in loads(k):
            copy.start()

    table_load.wait()
    ext[...] = jnp.broadcast_to(table_ref[:, TABLE_LEN - 1 : TABLE_LEN], (HEADS, 512))
    ext[:, 0:TABLE_LEN] = table_ref[...]
    ext[...] = pltpu.roll(ext[...], 65, 1) * LOG2E
    key_row = lax.broadcasted_iota(jnp.int32, (HALF, HALF), 0)
    query_col = lax.broadcasted_iota(jnp.int32, (HALF, HALF), 1)
    near_off = (key_row >= SEG_LEN) & (query_col < SEG_LEN)
    far_off = (key_row < SEG_LEN) & (query_col >= SEG_LEN)

    @pl.loop(0, HEADS)
    def _(h):
        row = ext[pl.ds(h, 1), :]
        for d in range(3):
            low = row[:, HALF * d : HALF * (d + 1)]
            high = row[:, HALF * (d + 1) : HALF * (d + 2)]
            around = jnp.broadcast_to(jnp.concatenate([high, low], axis=1), (HALF, 2 * HALF))
            tile = pltpu.roll(around, 0, 1, stride=1, stride_axis=0)[:, :HALF]
            if d == 0:
                tile = jnp.where(near_off, -FAR, tile)
            bias[h, d] = tile
        flat = jnp.broadcast_to(row[:, 511:512], (HALF, HALF))
        bias[h, 3] = flat
        bias[h, 4] = jnp.where(far_off, -FAR, flat)

    pl.semaphore_wait(barrier, greeted)

    def await_loads(k):
        for copy in loads(k):
            copy.wait()

    def send_kv(k):
        @pl.when(has_nxt)
        def _():
            kv_copy(k, 0).start()

    def send_qg(k):
        @pl.when(has_prv)
        def _():
            qg_copy(HEADS - 1 - k, 0).start()

    for copy in stat_loads:
        copy.wait()

    @pl.when(has_prv)
    def _():
        st_copy(0).start()

    for k in range(2):
        await_loads(k)
        send_kv(k)
        send_qg(k)
    pl.loop(2, HEADS)(await_loads)

    def clear(buffer, start, rows):
        @pl.loop(0, HEADS)
        def _(h):
            for n in range(2):
                buffer[h, n, start : start + rows, :] = jnp.zeros((rows, HEAD_DIM), BF16)

    @pl.when(jnp.logical_not(has_prv))
    def _():
        pl.loop(2, HEADS)(send_kv)
        clear(kv, 0, 2 * ROWS)

    @pl.when(jnp.logical_not(has_nxt))
    def _():
        pl.loop(2, HEADS)(send_qg)
        clear(qg, ROWS, 2 * ROWS)
        stats[1] = jnp.zeros((2 * HEADS, ROWS), F32)
        stats[2] = jnp.zeros((2 * HEADS, ROWS), F32)

    @pl.when(me == 1)
    def _():
        clear(kv, 0, ROWS)

    @pl.when(me + 2 == total)
    def _():
        clear(qg, 2 * ROWS, ROWS)
        stats[2] = jnp.zeros((2 * HEADS, ROWS), F32)

    @pl.when(has_nxt)
    def _():
        st_copy(0).wait_recv()

        @pl.when(has_prv)
        def _():
            st_copy(1).start()

    @pl.when(has_nxt2)
    def _():
        st_copy(1).wait_recv()

    def off(cond):
        return jnp.where(cond, FAR, 0.0).astype(F32)

    key_off = [off(me < 0), off(me < 1), off(me < 2)]
    query_off = [off(me < 0), off(me + 1 >= total), off(me + 2 >= total)]
    for lag in range(3):
        for n in range(2 * HEADS):
            row = stats[lag, n : n + 1, :]
            if n < HEADS:
                row = row * LOG2E + query_off[lag]
            wide[lag, n] = jnp.broadcast_to(row, (8, ROWS))

    def tile_terms(scores, weight_grads, bias_tile, log_row, dot_row):
        weights = jnp.exp2(scores * (inv_root * LOG2E) + (bias_tile - log_row))
        return weights, weights * (weight_grads - dot_row)

    def add_to(side, part, d, score_grads):
        if part == 0:
            acc[side, d] = score_grads
        else:
            acc[side, d] += score_grads

    def query_side(h):
        for part in range(2):
            rows = pl.ds(part * HALF, HALF)
            queries, grads = qg[h, 0, rows, :], qg[h, 1, rows, :]
            keys = kv[h, 0, pl.ds(part * HALF, BAND), :]
            values = kv[h, 1, pl.ds(part * HALF, BAND), :]
            scores = dot_nt(keys, queries)
            weight_grads = dot_nt(values, grads)
            log_row = wide[0, h, 0:1, rows]
            dot_row = wide[0, HEADS + h, 0:1, rows]
            pieces = []
            for t in range(5):
                d, lag = 4 - t, 2 - (part + t) // 2
                cut = slice(t * HALF, (t + 1) * HALF)
                _, score_grads = tile_terms(
                    scores[cut], weight_grads[cut], bias[h, d], log_row + key_off[lag], dot_row
                )
                add_to(0, part, d, score_grads)
                pieces.append(score_grads.astype(BF16))
            total_grads = dot_tn(jnp.concatenate(pieces, axis=0), keys)
            dq_ref[rows, cols_of(h)] = (total_grads * inv_root).astype(BF16)

    def key_side(h):
        for part in range(2):
            rows = pl.ds(part * HALF, HALF)
            own = pl.ds(512 + part * HALF, HALF)
            keys, values = kv[h, 0, own, :], kv[h, 1, own, :]
            queries = qg[h, 0, pl.ds(part * HALF, BAND), :]
            grads = qg[h, 1, pl.ds(part * HALF, BAND), :]
            scores = dot_nt(keys, queries)
            weight_grads = dot_nt(values, grads)
            score_pieces, weight_pieces = [], []
            for d in range(5):
                lag, cols = (part + d) // 2, pl.ds((part + d) % 2 * HALF, HALF)
                cut = slice(d * HALF, (d + 1) * HALF)
                log_row = wide[lag, h, 0:1, cols]
                dot_row = wide[lag, HEADS + h, 0:1, cols]
                weights, score_grads = tile_terms(
                    scores[:, cut], weight_grads[:, cut], bias[h, d], log_row, dot_row
                )
                add_to(1, part, d, score_grads)
                score_pieces.append(score_grads.astype(BF16))
                weight_pieces.append(weights.astype(BF16))
            key_grads = dot_nn(jnp.concatenate(score_pieces, axis=1), queries)
            dk_ref[rows, cols_of(h)] = (key_grads * inv_root).astype(BF16)
            value_grads = dot_nn(jnp.concatenate(weight_pieces, axis=1), grads)
            dv_ref[rows, cols_of(h)] = value_grads.astype(BF16)

    def table_row(side, h):
        zeros = jnp.zeros((HALF, HALF), F32)
        part = jnp.concatenate([acc[side, 0], acc[side, 1], acc[side, 2], zeros], axis=1)
        for step in (64, 32, 16, 8):
            part = part[:step] + pltpu.roll(part[step:], 512 - step, 1)
        row_id = lax.broadcasted_iota(jnp.int32, (8, 512), 0)
        for step in (4, 2, 1):
            moved = pltpu.roll(part, 512 - step, 1)
            part = jnp.where((row_id & step) != 0, moved, part)
        far = jnp.sum(acc[side, 3] + acc[side, 4], keepdims=True)
        by_distance = pltpu.roll(jnp.sum(part, axis=0, keepdims=True), SEG_LEN - 1, 1)
        lane = lax.broadcasted_iota(jnp.int32, (1, 512), 1)
        top = TABLE_LEN - 1
        clipped = (lane >= top) & (lane < 448)
        far = far + jnp.sum(jnp.where(clipped, by_distance, 0.0), keepdims=True)
        row = jnp.where(lane < top, by_distance, jnp.where(lane == top, far, 0.0))
        for n in range(4):
            tab[h, n : n + 1, :] = row[:, n * HALF : (n + 1) * HALF]

    def forward(k):
        @pl.when(has_prv)
        def _():
            kv_copy(k, 0).wait_recv()

            @pl.when(has_nxt)
            def _():
                kv_copy(k, 1).start()

        @pl.when(has_nxt)
        def _():
            qg_copy(HEADS - 1 - k, 0).wait_recv()

            @pl.when(has_prv)
            def _():
                qg_copy(HEADS - 1 - k, 1).start()

    def send_own(k):
        @pl.when(has_prv)
        def _():
            send_kv(k)

        @pl.when(has_nxt)
        def _():
            send_qg(k)

    @pl.loop(0, HEADS + 1)
    def _(k):
        in_round(0, k < y_rounds, tell)
        in_round(1, 2 * k < z_rounds, tell)

        @pl.when(k < GROUP)
        def _():
            forward(k)

        @pl.when(k < 2)
        def _():
            send_own(k + 2)

        @pl.when(k == GROUP - 1)
        def _():
            pl.loop(GROUP, HEADS)(send_own)

        in_round(1, 2 * k < z_rounds, hear)
        in_round(1, 2 * k + 1 < z_rounds, tell)

        @pl.when(k >= 1)
        def _():
            ahead, back = k - 1, HEADS - k

            @pl.when(has_prv2)
            def _():
                kv_copy(ahead, 1).wait_recv()

            query_side(ahead)

            @pl.when(k == HEADS - 1)
            def _():
                over_row.start(over_z.total())

            @pl.when(has_nxt2)
            def _():
                qg_copy(back, 1).wait_recv()

            key_side(back)

            @pl.when(k <= GROUP)
            def _():
                table_row(0, ahead)
                table_row(1, back)

        in_round(0, k < y_rounds, hear)
        in_round(1, 2 * k + 1 < z_rounds, hear)

        @pl.when(k == GROUP)
        def _():
            for h in range(HEADS):
                half, row = h // GROUP, 3 * (h % GROUP)
                tab_half[half, row : row + 3, :] = tab[h, 0:3, :]
            core_copy.start()
            core_copy.wait_recv()
            over_y.start(tab_half[at_core] + tab_core[...])
            pl.loop(GROUP, 6)(forward)
            over_z.start(over_y.total())
            pl.loop(6, HEADS)(forward)

    over_row.receive()
    for half in range(2):
        value = tab_row[half * tp_size]
        for x in range(1, tp_size):
            value = value + tab_row[half * tp_size + x]
        for h in range(GROUP):
            for n in range(3):
                width = min(HALF, TABLE_LEN - n * HALF)
                gt_ref[
                    half * GROUP + h : half * GROUP + h + 1, n * HALF : n * HALF + width
                ] = value[3 * h + n : 3 * h + n + 1, :width]

    @pl.when(has_nxt)
    def _():
        @pl.loop(0, HEADS)
        def _(h):
            kv_copy(h, 0).wait_send()

            @pl.when(has_prv)
            def _():
                kv_copy(h, 1).wait_send()

    @pl.when(has_prv)
    def _():
        st_copy(0).wait_send()

        @pl.when(has_nxt)
        def _():
            st_copy(1).wait_send()

        @pl.loop(0, HEADS)
        def _(h):
            qg_copy(h, 0).wait_send()

            @pl.when(has_nxt)
            def _():
                qg_copy(h, 1).wait_send()

    core_copy.wait_send()
    for line in (over_y, over_z, over_row):
        line.finish()


def write_out(*refs):
    count = len(refs) // 2
    copies = [
        pltpu.make_async_copy(refs[n], refs[count + n], refs[-1].at[n]) for n in range(count)
    ]
    for copy in copies:
        copy.start()
    for copy in copies:
        copy.wait()


def solution(mesh):
    sp_size, tp_size = mesh.shape["sp"], mesh.shape["tp"]

    def local(query_rows, key_rows, value_rows, out_grad, log_totals, out_dot, bias_table):
        hbm = pl.BlockSpec(memory_space=pltpu.HBM)
        z_size, y_size, core_size = SP_SHAPE
        tiles = (3 * GROUP, HALF)

        def in_hbm(array):
            return pltpu.with_memory_space_constraint(array, pltpu.HBM)

        vmem = pl.BlockSpec(memory_space=pltpu.VMEM)
        rows = jax.ShapeDtypeStruct(query_rows.shape, BF16)
        shapes = (rows, rows, rows, jax.ShapeDtypeStruct(bias_table.shape, F32))
        results = pl.pallas_call(
            functools.partial(kernel, sp_size, tp_size),
            out_shape=shapes,
            in_specs=[hbm] * 7,
            out_specs=(vmem, vmem, vmem, vmem),
            scratch_shapes=[
                pltpu.VMEM((HEADS, 2, 3 * ROWS, HEAD_DIM), BF16),
                pltpu.VMEM((HEADS, 2, 3 * ROWS, HEAD_DIM), BF16),
                pltpu.VMEM((3, 2 * HEADS, ROWS), F32),
                pltpu.VMEM((3, 2 * HEADS, 8, ROWS), F32),
                pltpu.VMEM((HEADS, 5, HALF, HALF), F32),
                pltpu.VMEM((HEADS, TABLE_LEN), F32),
                pltpu.VMEM((HEADS, 512), F32),
                pltpu.VMEM((2, 5, HALF, HALF), F32),
                pltpu.VMEM((HEADS, 4, HALF), F32),
                pltpu.VMEM((2,) + tiles, F32),
                pltpu.VMEM(tiles, F32),
                pltpu.VMEM((y_size,) + tiles, F32),
                pltpu.VMEM((z_size,) + tiles, F32),
                pltpu.VMEM((core_size * tp_size,) + tiles, F32),
                pltpu.SemaphoreType.DMA((4, HEADS)),
                pltpu.SemaphoreType.DMA((3,)),
                pltpu.SemaphoreType.REGULAR((4,)),
                pltpu.SemaphoreType.DMA((2,)),
                pltpu.SemaphoreType.DMA((y_size,)),
                pltpu.SemaphoreType.DMA((y_size,)),
                pltpu.SemaphoreType.DMA((z_size,)),
                pltpu.SemaphoreType.DMA((z_size,)),
                pltpu.SemaphoreType.DMA((core_size * tp_size,)),
                pltpu.SemaphoreType.DMA((core_size * tp_size,)),
                pltpu.SemaphoreType.DMA((2, HEADS)),
                pltpu.SemaphoreType.DMA((2, HEADS)),
                pltpu.SemaphoreType.DMA((2, HEADS)),
                pltpu.SemaphoreType.DMA((2, HEADS)),
                pltpu.SemaphoreType.DMA((2,)),
                pltpu.SemaphoreType.DMA((2,)),
            ],
            compiler_params=pltpu.CompilerParams(
                collective_id=0, has_side_effects=True, vmem_limit_bytes=32 * 2**20
            ),
        )(*map(in_hbm, (query_rows, key_rows, value_rows, out_grad, log_totals.T, out_dot.T, bias_table)))
        return pl.pallas_call(
            write_out,
            out_shape=shapes,
            in_specs=[vmem] * 4,
            out_specs=(hbm,) * 4,
            scratch_shapes=[pltpu.SemaphoreType.DMA((4,))],
        )(*(pltpu.with_memory_space_constraint(part, pltpu.VMEM) for part in results))

    split = P(("sp", "tp"), None)
    return jax.shard_map(
        local,
        mesh=mesh,
        in_specs=(split,) * 6 + (P(),),
        out_specs=(split, split, split, P()),
        check_vma=False,
    )
```

```python
import functools
import math

import jax
import jax.numpy as jnp
from jax import lax
from jax.experimental import pallas as pl
from jax.experimental.pallas import tpu as pltpu
from jax.sharding import PartitionSpec as P

SEG_LEN = 64
REL_CLIP = 256
ROWS = 256
HALF = 128
BAND = 640
HEADS = 8
HEAD_DIM = 128
TABLE_LEN = 320
LOG2E = math.log2(math.e)
FAR = 1e30
SP_SHAPE = (12, 8, 2)
GROUP = HEADS // 2
MESH = pl.DeviceIdType.MESH
F32 = jnp.float32
BF16 = jnp.bfloat16


def dot_nt(lhs, rhs):
    return lax.dot_general(lhs, rhs, (((1,), (1,)), ((), ())), preferred_element_type=F32)


def dot_nn(lhs, rhs):
    return lax.dot_general(lhs, rhs, (((1,), (0,)), ((), ())), preferred_element_type=F32)


def dot_tn(lhs, rhs):
    return lax.dot_general(lhs, rhs, (((0,), (0,)), ((), ())), preferred_element_type=F32)


def kernel(
    sp_size,
    tp_size,
    q_hbm,
    k_hbm,
    v_hbm,
    g_hbm,
    lse_hbm,
    dot_hbm,
    table_hbm,
    dq_ref,
    dk_ref,
    dv_ref,
    gt_ref,
    kv,
    qg,
    stats,
    wide,
    bias,
    table_ref,
    ext,
    acc,
    tab,
    tab_half,
    tab_core,
    tab_y,
    tab_z,
    tab_row,
    load_sem,
    stat_sem,
    chain,
    core_sem,
    y_send,
    y_recv,
    z_send,
    z_recv,
    row_send,
    row_recv,
    kv_send,
    kv_recv,
    qg_send,
    qg_recv,
    st_send,
    st_recv,
):
    sp, tp = lax.axis_index("sp"), lax.axis_index("tp")
    last_tp, first_tp = tp == tp_size - 1, tp == 0
    nxt = (
        lax.rem(sp + jnp.where(last_tp, 1, 0), sp_size),
        lax.rem(tp + 1, tp_size),
    )
    prv = (
        lax.rem(sp + sp_size - jnp.where(first_tp, 1, 0), sp_size),
        lax.rem(tp + tp_size - 1, tp_size),
    )
    z_size, y_size, core_size = SP_SHAPE
    at_z, at_y, at_core = sp // (y_size * core_size), sp // core_size % y_size, sp % core_size

    def at(z, y, core):
        return ((z * y_size + y) * core_size + core, tp)

    me = sp * tp_size + tp
    total = sp_size * tp_size
    inv_root = HEAD_DIM**-0.5

    def cols_of(h):
        return pl.ds(pl.multiple_of(h * HEAD_DIM, HEAD_DIM), HEAD_DIM)

    def loads(k):
        ahead, back = k, HEADS - 1 - k
        places = [
            (k_hbm, kv.at[ahead, 0, pl.ds(512, ROWS)], ahead),
            (v_hbm, kv.at[ahead, 1, pl.ds(512, ROWS)], ahead),
            (q_hbm, qg.at[back, 0, pl.ds(0, ROWS)], back),
            (g_hbm, qg.at[back, 1, pl.ds(0, ROWS)], back),
        ]
        return [
            pltpu.make_async_copy(
                src.at[:, cols_of(h)],
                dst,
                load_sem.at[n, h],
            )
            for n, (src, dst, h) in enumerate(places)
        ]

    def kv_copy(h, lag):
        src, dst = (512, 256) if lag == 0 else (256, 0)
        return pltpu.make_async_remote_copy(
            src_ref=kv.at[h, :, pl.ds(src, ROWS)],
            dst_ref=kv.at[h, :, pl.ds(dst, ROWS)],
            send_sem=kv_send.at[lag, h],
            recv_sem=kv_recv.at[lag, h],
            device_id=nxt,
            device_id_type=MESH,
        )

    def qg_copy(h, lag):
        return pltpu.make_async_remote_copy(
            src_ref=qg.at[h, :, pl.ds(lag * ROWS, ROWS)],
            dst_ref=qg.at[h, :, pl.ds((lag + 1) * ROWS, ROWS)],
            send_sem=qg_send.at[lag, h],
            recv_sem=qg_recv.at[lag, h],
            device_id=prv,
            device_id_type=MESH,
        )

    def st_copy(lag):
        return pltpu.make_async_remote_copy(
            src_ref=stats.at[lag],
            dst_ref=stats.at[lag + 1],
            send_sem=st_send.at[lag],
            recv_sem=st_recv.at[lag],
            device_id=prv,
            device_id_type=MESH,
        )

    class Exchange:
        def __init__(self, slots, size, mine, device, send, recv):
            self.slots, self.size, self.mine = slots, size, mine
            self.device, self.send, self.recv = device, send, recv

        def other(self, step):
            return lax.rem(self.mine + step, self.size)

        def copy(self, step, slot):
            return pltpu.make_async_remote_copy(
                src_ref=self.slots.at[slot],
                dst_ref=self.slots.at[slot],
                send_sem=self.send.at[step],
                recv_sem=self.recv.at[slot],
                device_id=self.device(self.other(step)),
                device_id_type=MESH,
            )

        def start(self, value):
            self.slots[self.mine] = value

            @pl.loop(1, self.size)
            def _(step):
                self.copy(step, self.mine).start()

        def receive(self):
            @pl.loop(1, self.size)
            def _(step):
                self.copy(step, self.other(step)).wait_recv()

        def total(self):
            self.receive()
            value = self.slots[0]
            for slot in range(1, self.size):
                value = value + self.slots[slot]
            return value

        def finish(self):
            @pl.loop(1, self.size)
            def _(step):
                self.copy(step, self.mine).wait_send()

    over_y = Exchange(tab_y, y_size, at_y, lambda y: at(at_z, y, at_core), y_send, y_recv)
    over_z = Exchange(tab_z, z_size, at_z, lambda z: at(z, at_y, at_core), z_send, z_recv)
    row_size = core_size * tp_size
    over_row = Exchange(
        tab_row,
        row_size,
        at_core * tp_size + tp,
        lambda e: (at(at_z, at_y, e // tp_size)[0], lax.rem(e, tp_size)),
        row_send,
        row_recv,
    )
    other_core = at(at_z, at_y, 1 - at_core)
    core_copy = pltpu.make_async_remote_copy(
        src_ref=tab_half.at[1 - at_core],
        dst_ref=tab_core,
        send_sem=core_sem.at[0],
        recv_sem=core_sem.at[1],
        device_id=other_core,
        device_id_type=MESH,
    )

    stat_loads = [
        pltpu.make_async_copy(lse_hbm, stats.at[0, pl.ds(0, HEADS)], stat_sem.at[0]),
        pltpu.make_async_copy(dot_hbm, stats.at[0, pl.ds(HEADS, HEADS)], stat_sem.at[1]),
    ]
    table_load = pltpu.make_async_copy(table_hbm, table_ref, stat_sem.at[2])

    has_prv, has_nxt = me >= 1, me + 1 < total
    has_prv2, has_nxt2 = me >= 2, me + 2 < total
    y_low, y_high = lax.rem(at_y + y_size - 1, y_size), lax.rem(at_y + 1, y_size)
    z_low, z_high = lax.rem(at_z + z_size - 1, z_size), lax.rem(at_z + 1, z_size)
    lines = (
        (at(at_z, y_low, at_core), at(at_z, y_high, at_core), y_size > 2, y_size > 1),
        (at(z_low, at_y, at_core), at(z_high, at_y, at_core), at_z > 0, at_z < z_size - 1),
    )
    near = [(nxt, has_nxt), (prv, has_prv)]
    near += [(over_row.device(over_row.other(step)), True) for step in range(1, row_size)]
    for low, high, has_low, has_high in lines:
        near += [(low, has_low), (high, has_high)]
    greeted = sum(jnp.where(cond, 1, 0) for _, cond in near)

    def tell(line):
        low, high, has_low, has_high = lines[line]

        @pl.when(has_low)
        def _():
            pl.semaphore_signal(
                chain.at[2 * line + 1], inc=1, device_id=low, device_id_type=MESH
            )

        @pl.when(has_high)
        def _():
            pl.semaphore_signal(chain.at[2 * line], inc=1, device_id=high, device_id_type=MESH)

    def hear(line):
        _, _, has_low, has_high = lines[line]

        @pl.when(has_low)
        def _():
            pl.semaphore_wait(chain.at[2 * line], 1)

        @pl.when(has_high)
        def _():
            pl.semaphore_wait(chain.at[2 * line + 1], 1)

    y_rounds, z_rounds = max(y_size // 2 - 1, 0), max(z_size - 2, 0)

    def in_round(line, cond, act):
        @pl.when(cond)
        def _():
            act(line)

    barrier = pltpu.get_barrier_semaphore()
    for device, cond in near:

        @pl.when(cond)
        def _():
            pl.semaphore_signal(barrier, inc=1, device_id=device, device_id_type=MESH)

    table_load.start()
    for copy in stat_loads:
        copy.start()

    @pl.loop(0, HEADS)
    def _(k):
        for copy in loads(k):
            copy.start()

    pl.semaphore_wait(barrier, greeted)

    def await_loads(k):
        for copy in loads(k):
            copy.wait()

    def send_kv(k):
        @pl.when(has_nxt)
        def _():
            kv_copy(k, 0).start()

    def send_qg(k):
        @pl.when(has_prv)
        def _():
            qg_copy(HEADS - 1 - k, 0).start()

    for copy in stat_loads:
        copy.wait()

    @pl.when(has_prv)
    def _():
        st_copy(0).start()

    for k in range(2):
        await_loads(k)
        send_kv(k)
        send_qg(k)
    pl.loop(2, HEADS)(await_loads)
    table_load.wait()
    ext[...] = jnp.broadcast_to(table_ref[:, TABLE_LEN - 1 : TABLE_LEN], (HEADS, 512))
    ext[:, 0:TABLE_LEN] = table_ref[...]
    ext[...] = pltpu.roll(ext[...], 65, 1) * LOG2E
    key_row = lax.broadcasted_iota(jnp.int32, (HALF, HALF), 0)
    query_col = lax.broadcasted_iota(jnp.int32, (HALF, HALF), 1)
    near_off = (key_row >= SEG_LEN) & (query_col < SEG_LEN)
    far_off = (key_row < SEG_LEN) & (query_col >= SEG_LEN)

    @pl.loop(0, HEADS)
    def _(h):
        row = ext[pl.ds(h, 1), :]
        for d in range(3):
            low = row[:, HALF * d : HALF * (d + 1)]
            high = row[:, HALF * (d + 1) : HALF * (d + 2)]
            around = jnp.broadcast_to(jnp.concatenate([high, low], axis=1), (HALF, 2 * HALF))
            tile = pltpu.roll(around, 0, 1, stride=1, stride_axis=0)[:, :HALF]
            if d == 0:
                tile = jnp.where(near_off, -FAR, tile)
            bias[h, d] = tile
        flat = jnp.broadcast_to(row[:, 511:512], (HALF, HALF))
        bias[h, 3] = flat
        bias[h, 4] = jnp.where(far_off, -FAR, flat)


    def clear(buffer, start, rows):
        @pl.loop(0, HEADS)
        def _(h):
            for n in range(2):
                buffer[h, n, start : start + rows, :] = jnp.zeros((rows, HEAD_DIM), BF16)

    @pl.when(jnp.logical_not(has_prv))
    def _():
        pl.loop(2, HEADS)(send_kv)
        clear(kv, 0, 2 * ROWS)

    @pl.when(jnp.logical_not(has_nxt))
    def _():
        pl.loop(2, HEADS)(send_qg)
        clear(qg, ROWS, 2 * ROWS)
        stats[1] = jnp.zeros((2 * HEADS, ROWS), F32)
        stats[2] = jnp.zeros((2 * HEADS, ROWS), F32)

    @pl.when(me == 1)
    def _():
        clear(kv, 0, ROWS)

    @pl.when(me + 2 == total)
    def _():
        clear(qg, 2 * ROWS, ROWS)
        stats[2] = jnp.zeros((2 * HEADS, ROWS), F32)

    @pl.when(has_nxt)
    def _():
        st_copy(0).wait_recv()

        @pl.when(has_prv)
        def _():
            st_copy(1).start()

    @pl.when(has_nxt2)
    def _():
        st_copy(1).wait_recv()

    def off(cond):
        return jnp.where(cond, FAR, 0.0).astype(F32)

    key_off = [off(me < 0), off(me < 1), off(me < 2)]
    query_off = [off(me < 0), off(me + 1 >= total), off(me + 2 >= total)]
    for lag in range(3):
        for n in range(2 * HEADS):
            row = stats[lag, n : n + 1, :]
            if n < HEADS:
                row = row * LOG2E + query_off[lag]
            wide[lag, n] = jnp.broadcast_to(row, (8, ROWS))

    def tile_terms(scores, weight_grads, bias_tile, log_row, dot_row):
        weights = jnp.exp2(scores * (inv_root * LOG2E) + (bias_tile - log_row))
        return weights, weights * (weight_grads - dot_row)

    def add_to(side, part, d, score_grads):
        if part == 0:
            acc[side, d] = score_grads
        else:
            acc[side, d] += score_grads

    def query_side(h):
        for part in range(2):
            rows = pl.ds(part * HALF, HALF)
            queries, grads = qg[h, 0, rows, :], qg[h, 1, rows, :]
            keys = kv[h, 0, pl.ds(part * HALF, BAND), :]
            values = kv[h, 1, pl.ds(part * HALF, BAND), :]
            scores = dot_nt(keys, queries)
            weight_grads = dot_nt(values, grads)
            log_row = wide[0, h, 0:1, rows]
            dot_row = wide[0, HEADS + h, 0:1, rows]
            pieces = []
            for t in range(5):
                d, lag = 4 - t, 2 - (part + t) // 2
                cut = slice(t * HALF, (t + 1) * HALF)
                _, score_grads = tile_terms(
                    scores[cut], weight_grads[cut], bias[h, d], log_row + key_off[lag], dot_row
                )
                add_to(0, part, d, score_grads)
                pieces.append(score_grads.astype(BF16))
            total_grads = dot_tn(jnp.concatenate(pieces, axis=0), keys)
            dq_ref[rows, cols_of(h)] = (total_grads * inv_root).astype(BF16)

    def key_side(h):
        for part in range(2):
            rows = pl.ds(part * HALF, HALF)
            own = pl.ds(512 + part * HALF, HALF)
            keys, values = kv[h, 0, own, :], kv[h, 1, own, :]
            queries = qg[h, 0, pl.ds(part * HALF, BAND), :]
            grads = qg[h, 1, pl.ds(part * HALF, BAND), :]
            scores = dot_nt(keys, queries)
            weight_grads = dot_nt(values, grads)
            score_pieces, weight_pieces = [], []
            for d in range(5):
                lag, cols = (part + d) // 2, pl.ds((part + d) % 2 * HALF, HALF)
                cut = slice(d * HALF, (d + 1) * HALF)
                log_row = wide[lag, h, 0:1, cols]
                dot_row = wide[lag, HEADS + h, 0:1, cols]
                weights, score_grads = tile_terms(
                    scores[:, cut], weight_grads[:, cut], bias[h, d], log_row, dot_row
                )
                add_to(1, part, d, score_grads)
                score_pieces.append(score_grads.astype(BF16))
                weight_pieces.append(weights.astype(BF16))
            key_grads = dot_nn(jnp.concatenate(score_pieces, axis=1), queries)
            dk_ref[rows, cols_of(h)] = (key_grads * inv_root).astype(BF16)
            value_grads = dot_nn(jnp.concatenate(weight_pieces, axis=1), grads)
            dv_ref[rows, cols_of(h)] = value_grads.astype(BF16)

    def table_row(side, h):
        zeros = jnp.zeros((HALF, HALF), F32)
        part = jnp.concatenate([acc[side, 0], acc[side, 1], acc[side, 2], zeros], axis=1)
        for step in (64, 32, 16, 8):
            part = part[:step] + pltpu.roll(part[step:], 512 - step, 1)
        row_id = lax.broadcasted_iota(jnp.int32, (8, 512), 0)
        for step in (4, 2, 1):
            moved = pltpu.roll(part, 512 - step, 1)
            part = jnp.where((row_id & step) != 0, moved, part)
        far = jnp.sum(acc[side, 3] + acc[side, 4], keepdims=True)
        by_distance = pltpu.roll(jnp.sum(part, axis=0, keepdims=True), SEG_LEN - 1, 1)
        lane = lax.broadcasted_iota(jnp.int32, (1, 512), 1)
        top = TABLE_LEN - 1
        clipped = (lane >= top) & (lane < 448)
        far = far + jnp.sum(jnp.where(clipped, by_distance, 0.0), keepdims=True)
        row = jnp.where(lane < top, by_distance, jnp.where(lane == top, far, 0.0))
        for n in range(4):
            tab[h, n : n + 1, :] = row[:, n * HALF : (n + 1) * HALF]

    def forward(k):
        @pl.when(has_prv)
        def _():
            kv_copy(k, 0).wait_recv()

            @pl.when(has_nxt)
            def _():
                kv_copy(k, 1).start()

        @pl.when(has_nxt)
        def _():
            qg_copy(HEADS - 1 - k, 0).wait_recv()

            @pl.when(has_prv)
            def _():
                qg_copy(HEADS - 1 - k, 1).start()

    def send_own(k):
        @pl.when(has_prv)
        def _():
            send_kv(k)

        @pl.when(has_nxt)
        def _():
            send_qg(k)

    @pl.loop(0, HEADS + 1)
    def _(k):
        in_round(0, k < y_rounds, tell)
        in_round(1, 2 * k < z_rounds, tell)

        @pl.when(k < GROUP)
        def _():
            forward(k)

        @pl.when(k < 2)
        def _():
            send_own(k + 2)

        @pl.when(k == GROUP - 1)
        def _():
            pl.loop(GROUP, 6)(send_own)

        in_round(1, 2 * k < z_rounds, hear)
        in_round(1, 2 * k + 1 < z_rounds, tell)

        @pl.when(k >= 1)
        def _():
            ahead, back = k - 1, HEADS - k

            @pl.when(has_prv2)
            def _():
                kv_copy(ahead, 1).wait_recv()

            query_side(ahead)

            @pl.when(k == HEADS - 1)
            def _():
                over_row.start(over_z.total())

            @pl.when(has_nxt2)
            def _():
                qg_copy(back, 1).wait_recv()

            key_side(back)

            @pl.when(k <= GROUP)
            def _():
                table_row(0, ahead)
                table_row(1, back)

        in_round(0, k < y_rounds, hear)
        in_round(1, 2 * k + 1 < z_rounds, hear)

        @pl.when(k == GROUP)
        def _():
            for h in range(HEADS):
                half, row = h // GROUP, 3 * (h % GROUP)
                tab_half[half, row : row + 3, :] = tab[h, 0:3, :]
            core_copy.start()
            forward(4)
            core_copy.wait_recv()
            over_y.start(tab_half[at_core] + tab_core[...])
            send_own(6)
            forward(5)
            over_z.start(over_y.total())
            send_own(7)
            pl.loop(6, HEADS)(forward)

    over_row.receive()
    for half in range(2):
        value = tab_row[half * tp_size]
        for x in range(1, tp_size):
            value = value + tab_row[half * tp_size + x]
        for h in range(GROUP):
            for n in range(3):
                width = min(HALF, TABLE_LEN - n * HALF)
                gt_ref[
                    half * GROUP + h : half * GROUP + h + 1, n * HALF : n * HALF + width
                ] = value[3 * h + n : 3 * h + n + 1, :width]

    @pl.when(has_nxt)
    def _():
        @pl.loop(0, HEADS)
        def _(h):
            kv_copy(h, 0).wait_send()

            @pl.when(has_prv)
            def _():
                kv_copy(h, 1).wait_send()

    @pl.when(has_prv)
    def _():
        st_copy(0).wait_send()

        @pl.when(has_nxt)
        def _():
            st_copy(1).wait_send()

        @pl.loop(0, HEADS)
        def _(h):
            qg_copy(h, 0).wait_send()

            @pl.when(has_nxt)
            def _():
                qg_copy(h, 1).wait_send()

    core_copy.wait_send()
    for line in (over_y, over_z, over_row):
        line.finish()


def write_out(*refs):
    count = len(refs) // 2
    copies = [
        pltpu.make_async_copy(refs[n], refs[count + n], refs[-1].at[n]) for n in range(count)
    ]
    for copy in copies:
        copy.start()
    for copy in copies:
        copy.wait()


def solution(mesh):
    sp_size, tp_size = mesh.shape["sp"], mesh.shape["tp"]

    def local(query_rows, key_rows, value_rows, out_grad, log_totals, out_dot, bias_table):
        hbm = pl.BlockSpec(memory_space=pltpu.HBM)
        z_size, y_size, core_size = SP_SHAPE
        tiles = (3 * GROUP, HALF)

        def in_hbm(array):
            return pltpu.with_memory_space_constraint(array, pltpu.HBM)

        vmem = pl.BlockSpec(memory_space=pltpu.VMEM)
        rows = jax.ShapeDtypeStruct(query_rows.shape, BF16)
        shapes = (rows, rows, rows, jax.ShapeDtypeStruct(bias_table.shape, F32))
        results = pl.pallas_call(
            functools.partial(kernel, sp_size, tp_size),
            out_shape=shapes,
            in_specs=[hbm] * 7,
            out_specs=(vmem, vmem, vmem, vmem),
            scratch_shapes=[
                pltpu.VMEM((HEADS, 2, 3 * ROWS, HEAD_DIM), BF16),
                pltpu.VMEM((HEADS, 2, 3 * ROWS, HEAD_DIM), BF16),
                pltpu.VMEM((3, 2 * HEADS, ROWS), F32),
                pltpu.VMEM((3, 2 * HEADS, 8, ROWS), F32),
                pltpu.VMEM((HEADS, 5, HALF, HALF), F32),
                pltpu.VMEM((HEADS, TABLE_LEN), F32),
                pltpu.VMEM((HEADS, 512), F32),
                pltpu.VMEM((2, 5, HALF, HALF), F32),
                pltpu.VMEM((HEADS, 4, HALF), F32),
                pltpu.VMEM((2,) + tiles, F32),
                pltpu.VMEM(tiles, F32),
                pltpu.VMEM((y_size,) + tiles, F32),
                pltpu.VMEM((z_size,) + tiles, F32),
                pltpu.VMEM((core_size * tp_size,) + tiles, F32),
                pltpu.SemaphoreType.DMA((4, HEADS)),
                pltpu.SemaphoreType.DMA((3,)),
                pltpu.SemaphoreType.REGULAR((4,)),
                pltpu.SemaphoreType.DMA((2,)),
                pltpu.SemaphoreType.DMA((y_size,)),
                pltpu.SemaphoreType.DMA((y_size,)),
                pltpu.SemaphoreType.DMA((z_size,)),
                pltpu.SemaphoreType.DMA((z_size,)),
                pltpu.SemaphoreType.DMA((core_size * tp_size,)),
                pltpu.SemaphoreType.DMA((core_size * tp_size,)),
                pltpu.SemaphoreType.DMA((2, HEADS)),
                pltpu.SemaphoreType.DMA((2, HEADS)),
                pltpu.SemaphoreType.DMA((2, HEADS)),
                pltpu.SemaphoreType.DMA((2, HEADS)),
                pltpu.SemaphoreType.DMA((2,)),
                pltpu.SemaphoreType.DMA((2,)),
            ],
            compiler_params=pltpu.CompilerParams(
                collective_id=0, has_side_effects=True, vmem_limit_bytes=32 * 2**20
            ),
        )(*map(in_hbm, (query_rows, key_rows, value_rows, out_grad, log_totals.T, out_dot.T, bias_table)))
        return pl.pallas_call(
            write_out,
            out_shape=shapes,
            in_specs=[vmem] * 4,
            out_specs=(hbm,) * 4,
            scratch_shapes=[pltpu.SemaphoreType.DMA((4,))],
        )(*(pltpu.with_memory_space_constraint(part, pltpu.VMEM) for part in results))

    split = P(("sp", "tp"), None)
    return jax.shard_map(
        local,
        mesh=mesh,
        in_specs=(split,) * 6 + (P(),),
        out_specs=(split, split, split, P()),
        check_vma=False,
    )
```

```python
import functools
import math

import jax
import jax.numpy as jnp
from jax import lax
from jax.experimental import pallas as pl
from jax.experimental.pallas import tpu as pltpu
from jax.sharding import PartitionSpec as P

SEG_LEN = 64
REL_CLIP = 256
ROWS = 256
HALF = 128
BAND = 640
HEADS = 8
HEAD_DIM = 128
TABLE_LEN = 320
LOG2E = math.log2(math.e)
FAR = 1e30
SP_SHAPE = (12, 8, 2)
GROUP = HEADS // 2
MESH = pl.DeviceIdType.MESH
F32 = jnp.float32
BF16 = jnp.bfloat16


def dot_nt(lhs, rhs):
    return lax.dot_general(lhs, rhs, (((1,), (1,)), ((), ())), preferred_element_type=F32)


def dot_nn(lhs, rhs):
    return lax.dot_general(lhs, rhs, (((1,), (0,)), ((), ())), preferred_element_type=F32)


def dot_tn(lhs, rhs):
    return lax.dot_general(lhs, rhs, (((0,), (0,)), ((), ())), preferred_element_type=F32)


def kernel(
    sp_size,
    tp_size,
    q_hbm,
    k_hbm,
    v_hbm,
    g_hbm,
    lse_hbm,
    dot_hbm,
    table_hbm,
    dq_ref,
    dk_ref,
    dv_ref,
    gt_ref,
    kv,
    qg,
    stats,
    wide,
    bias,
    table_ref,
    ext,
    acc,
    tab,
    tab_half,
    tab_core,
    tab_y,
    tab_z,
    tab_row,
    load_sem,
    stat_sem,
    chain,
    core_sem,
    y_send,
    y_recv,
    z_send,
    z_recv,
    row_send,
    row_recv,
    kv_send,
    kv_recv,
    qg_send,
    qg_recv,
    st_send,
    st_recv,
):
    sp, tp = lax.axis_index("sp"), lax.axis_index("tp")
    last_tp, first_tp = tp == tp_size - 1, tp == 0
    nxt = (
        lax.rem(sp + jnp.where(last_tp, 1, 0), sp_size),
        lax.rem(tp + 1, tp_size),
    )
    prv = (
        lax.rem(sp + sp_size - jnp.where(first_tp, 1, 0), sp_size),
        lax.rem(tp + tp_size - 1, tp_size),
    )
    z_size, y_size, core_size = SP_SHAPE
    at_z, at_y, at_core = sp // (y_size * core_size), sp // core_size % y_size, sp % core_size

    def at(z, y, core):
        return ((z * y_size + y) * core_size + core, tp)

    me = sp * tp_size + tp
    total = sp_size * tp_size
    inv_root = HEAD_DIM**-0.5

    def cols_of(h):
        return pl.ds(pl.multiple_of(h * HEAD_DIM, HEAD_DIM), HEAD_DIM)

    def loads(k):
        ahead, back = k, HEADS - 1 - k
        places = [
            (k_hbm, kv.at[ahead, 0, pl.ds(512, ROWS)], ahead),
            (v_hbm, kv.at[ahead, 1, pl.ds(512, ROWS)], ahead),
            (q_hbm, qg.at[back, 0, pl.ds(0, ROWS)], back),
            (g_hbm, qg.at[back, 1, pl.ds(0, ROWS)], back),
        ]
        return [
            pltpu.make_async_copy(
                src.at[:, cols_of(h)],
                dst,
                load_sem.at[n, h],
            )
            for n, (src, dst, h) in enumerate(places)
        ]

    def kv_copy(h, lag):
        src, dst = (512, 256) if lag == 0 else (256, 0)
        return pltpu.make_async_remote_copy(
            src_ref=kv.at[h, :, pl.ds(src, ROWS)],
            dst_ref=kv.at[h, :, pl.ds(dst, ROWS)],
            send_sem=kv_send.at[lag, h],
            recv_sem=kv_recv.at[lag, h],
            device_id=nxt,
            device_id_type=MESH,
        )

    def qg_copy(h, lag):
        return pltpu.make_async_remote_copy(
            src_ref=qg.at[h, :, pl.ds(lag * ROWS, ROWS)],
            dst_ref=qg.at[h, :, pl.ds((lag + 1) * ROWS, ROWS)],
            send_sem=qg_send.at[lag, h],
            recv_sem=qg_recv.at[lag, h],
            device_id=prv,
            device_id_type=MESH,
        )

    def st_copy(lag):
        return pltpu.make_async_remote_copy(
            src_ref=stats.at[lag],
            dst_ref=stats.at[lag + 1],
            send_sem=st_send.at[lag],
            recv_sem=st_recv.at[lag],
            device_id=prv,
            device_id_type=MESH,
        )

    class Exchange:
        def __init__(self, slots, size, mine, device, send, recv):
            self.slots, self.size, self.mine = slots, size, mine
            self.device, self.send, self.recv = device, send, recv

        def other(self, step):
            return lax.rem(self.mine + step, self.size)

        def copy(self, step, slot):
            return pltpu.make_async_remote_copy(
                src_ref=self.slots.at[slot],
                dst_ref=self.slots.at[slot],
                send_sem=self.send.at[step],
                recv_sem=self.recv.at[slot],
                device_id=self.device(self.other(step)),
                device_id_type=MESH,
            )

        def start(self, value):
            self.slots[self.mine] = value

            @pl.loop(1, self.size)
            def _(step):
                self.copy(step, self.mine).start()

        def receive(self):
            @pl.loop(1, self.size)
            def _(step):
                self.copy(step, self.other(step)).wait_recv()

        def total(self):
            self.receive()
            value = self.slots[0]
            for slot in range(1, self.size):
                value = value + self.slots[slot]
            return value

        def finish(self):
            @pl.loop(1, self.size)
            def _(step):
                self.copy(step, self.mine).wait_send()

    over_y = Exchange(tab_y, y_size, at_y, lambda y: at(at_z, y, at_core), y_send, y_recv)
    over_z = Exchange(tab_z, z_size, at_z, lambda z: at(z, at_y, at_core), z_send, z_recv)
    row_size = core_size * tp_size
    over_row = Exchange(
        tab_row,
        row_size,
        at_core * tp_size + tp,
        lambda e: (at(at_z, at_y, e // tp_size)[0], lax.rem(e, tp_size)),
        row_send,
        row_recv,
    )
    other_core = at(at_z, at_y, 1 - at_core)
    core_copy = pltpu.make_async_remote_copy(
        src_ref=tab_half.at[1 - at_core],
        dst_ref=tab_core,
        send_sem=core_sem.at[0],
        recv_sem=core_sem.at[1],
        device_id=other_core,
        device_id_type=MESH,
    )

    stat_loads = [
        pltpu.make_async_copy(lse_hbm, stats.at[0, pl.ds(0, HEADS)], stat_sem.at[0]),
        pltpu.make_async_copy(dot_hbm, stats.at[0, pl.ds(HEADS, HEADS)], stat_sem.at[1]),
    ]
    table_load = pltpu.make_async_copy(table_hbm, table_ref, stat_sem.at[2])

    has_prv, has_nxt = me >= 1, me + 1 < total
    has_prv2, has_nxt2 = me >= 2, me + 2 < total
    y_low, y_high = lax.rem(at_y + y_size - 1, y_size), lax.rem(at_y + 1, y_size)
    z_low, z_high = lax.rem(at_z + z_size - 1, z_size), lax.rem(at_z + 1, z_size)
    lines = (
        (at(at_z, y_low, at_core), at(at_z, y_high, at_core), y_size > 2, y_size > 1),
        (at(z_low, at_y, at_core), at(z_high, at_y, at_core), at_z > 0, at_z < z_size - 1),
        (prv, nxt, has_prv, has_nxt),
    )
    near = [(nxt, has_nxt), (prv, has_prv)]
    for low, high, has_low, has_high in lines[:2]:
        near += [(low, has_low), (high, has_high)]
    greeted = sum(jnp.where(cond, 1, 0) for _, cond in near)

    def tell(line):
        low, high, has_low, has_high = lines[line]

        @pl.when(has_low)
        def _():
            pl.semaphore_signal(
                chain.at[2 * line + 1], inc=1, device_id=low, device_id_type=MESH
            )

        @pl.when(has_high)
        def _():
            pl.semaphore_signal(chain.at[2 * line], inc=1, device_id=high, device_id_type=MESH)

    def hear(line):
        _, _, has_low, has_high = lines[line]

        @pl.when(has_low)
        def _():
            pl.semaphore_wait(chain.at[2 * line], 1)

        @pl.when(has_high)
        def _():
            pl.semaphore_wait(chain.at[2 * line + 1], 1)

    y_rounds, z_rounds = max(y_size // 2 - 1, 0), max(z_size - 2, 0)

    def in_round(line, cond, act):
        @pl.when(cond)
        def _():
            act(line)

    barrier = pltpu.get_barrier_semaphore()
    for device, cond in near:

        @pl.when(cond)
        def _():
            pl.semaphore_signal(barrier, inc=1, device_id=device, device_id_type=MESH)

    table_load.start()
    for copy in stat_loads:
        copy.start()

    @pl.loop(0, HEADS)
    def _(k):
        for copy in loads(k):
            copy.start()

    pl.semaphore_wait(barrier, greeted)

    def await_loads(k):
        for copy in loads(k):
            copy.wait()

    def send_kv(k):
        @pl.when(has_nxt)
        def _():
            kv_copy(k, 0).start()

    def send_qg(k):
        @pl.when(has_prv)
        def _():
            qg_copy(HEADS - 1 - k, 0).start()

    for copy in stat_loads:
        copy.wait()

    @pl.when(has_prv)
    def _():
        st_copy(0).start()

    for k in range(2):
        await_loads(k)
        send_kv(k)
        send_qg(k)
    pl.loop(2, HEADS)(await_loads)
    table_load.wait()
    ext[...] = jnp.broadcast_to(table_ref[:, TABLE_LEN - 1 : TABLE_LEN], (HEADS, 512))
    ext[:, 0:TABLE_LEN] = table_ref[...]
    ext[...] = pltpu.roll(ext[...], 65, 1) * LOG2E
    key_row = lax.broadcasted_iota(jnp.int32, (HALF, HALF), 0)
    query_col = lax.broadcasted_iota(jnp.int32, (HALF, HALF), 1)
    near_off = (key_row >= SEG_LEN) & (query_col < SEG_LEN)
    far_off = (key_row < SEG_LEN) & (query_col >= SEG_LEN)

    @pl.loop(0, HEADS)
    def _(h):
        row = ext[pl.ds(h, 1), :]
        for d in range(3):
            low = row[:, HALF * d : HALF * (d + 1)]
            high = row[:, HALF * (d + 1) : HALF * (d + 2)]
            around = jnp.broadcast_to(jnp.concatenate([high, low], axis=1), (HALF, 2 * HALF))
            tile = pltpu.roll(around, 0, 1, stride=1, stride_axis=0)[:, :HALF]
            if d == 0:
                tile = jnp.where(near_off, -FAR, tile)
            bias[h, d] = tile
        flat = jnp.broadcast_to(row[:, 511:512], (HALF, HALF))
        bias[h, 3] = flat
        bias[h, 4] = jnp.where(far_off, -FAR, flat)


    def clear(buffer, start, rows):
        @pl.loop(0, HEADS)
        def _(h):
            for n in range(2):
                buffer[h, n, start : start + rows, :] = jnp.zeros((rows, HEAD_DIM), BF16)

    @pl.when(jnp.logical_not(has_prv))
    def _():
        pl.loop(2, HEADS)(send_kv)
        clear(kv, 0, 2 * ROWS)

    @pl.when(jnp.logical_not(has_nxt))
    def _():
        pl.loop(2, HEADS)(send_qg)
        clear(qg, ROWS, 2 * ROWS)
        stats[1] = jnp.zeros((2 * HEADS, ROWS), F32)
        stats[2] = jnp.zeros((2 * HEADS, ROWS), F32)

    @pl.when(me == 1)
    def _():
        clear(kv, 0, ROWS)

    @pl.when(me + 2 == total)
    def _():
        clear(qg, 2 * ROWS, ROWS)
        stats[2] = jnp.zeros((2 * HEADS, ROWS), F32)

    @pl.when(has_nxt)
    def _():
        st_copy(0).wait_recv()

        @pl.when(has_prv)
        def _():
            st_copy(1).start()

    @pl.when(has_nxt2)
    def _():
        st_copy(1).wait_recv()

    def off(cond):
        return jnp.where(cond, FAR, 0.0).astype(F32)

    key_off = [off(me < 0), off(me < 1), off(me < 2)]
    query_off = [off(me < 0), off(me + 1 >= total), off(me + 2 >= total)]
    for lag in range(3):
        for n in range(2 * HEADS):
            row = stats[lag, n : n + 1, :]
            if n < HEADS:
                row = row * LOG2E + query_off[lag]
            wide[lag, n] = jnp.broadcast_to(row, (8, ROWS))

    def tile_terms(scores, weight_grads, bias_tile, log_row, dot_row):
        weights = jnp.exp2(scores * (inv_root * LOG2E) + (bias_tile - log_row))
        return weights, weights * (weight_grads - dot_row)

    def add_to(side, part, d, score_grads):
        if part == 0:
            acc[side, d] = score_grads
        else:
            acc[side, d] += score_grads

    def query_side(h):
        for part in range(2):
            rows = pl.ds(part * HALF, HALF)
            queries, grads = qg[h, 0, rows, :], qg[h, 1, rows, :]
            keys = kv[h, 0, pl.ds(part * HALF, BAND), :]
            values = kv[h, 1, pl.ds(part * HALF, BAND), :]
            scores = dot_nt(keys, queries)
            weight_grads = dot_nt(values, grads)
            log_row = wide[0, h, 0:1, rows]
            dot_row = wide[0, HEADS + h, 0:1, rows]
            pieces = []
            for t in range(5):
                d, lag = 4 - t, 2 - (part + t) // 2
                cut = slice(t * HALF, (t + 1) * HALF)
                _, score_grads = tile_terms(
                    scores[cut], weight_grads[cut], bias[h, d], log_row + key_off[lag], dot_row
                )
                add_to(0, part, d, score_grads)
                pieces.append(score_grads.astype(BF16))
            total_grads = dot_tn(jnp.concatenate(pieces, axis=0), keys)
            dq_ref[rows, cols_of(h)] = (total_grads * inv_root).astype(BF16)

    def key_side(h):
        for part in range(2):
            rows = pl.ds(part * HALF, HALF)
            own = pl.ds(512 + part * HALF, HALF)
            keys, values = kv[h, 0, own, :], kv[h, 1, own, :]
            queries = qg[h, 0, pl.ds(part * HALF, BAND), :]
            grads = qg[h, 1, pl.ds(part * HALF, BAND), :]
            scores = dot_nt(keys, queries)
            weight_grads = dot_nt(values, grads)
            score_pieces, weight_pieces = [], []
            for d in range(5):
                lag, cols = (part + d) // 2, pl.ds((part + d) % 2 * HALF, HALF)
                cut = slice(d * HALF, (d + 1) * HALF)
                log_row = wide[lag, h, 0:1, cols]
                dot_row = wide[lag, HEADS + h, 0:1, cols]
                weights, score_grads = tile_terms(
                    scores[:, cut], weight_grads[:, cut], bias[h, d], log_row, dot_row
                )
                add_to(1, part, d, score_grads)
                score_pieces.append(score_grads.astype(BF16))
                weight_pieces.append(weights.astype(BF16))
            key_grads = dot_nn(jnp.concatenate(score_pieces, axis=1), queries)
            dk_ref[rows, cols_of(h)] = (key_grads * inv_root).astype(BF16)
            value_grads = dot_nn(jnp.concatenate(weight_pieces, axis=1), grads)
            dv_ref[rows, cols_of(h)] = value_grads.astype(BF16)

    def table_row(side, h):
        zeros = jnp.zeros((HALF, HALF), F32)
        part = jnp.concatenate([acc[side, 0], acc[side, 1], acc[side, 2], zeros], axis=1)
        for step in (64, 32, 16, 8):
            part = part[:step] + pltpu.roll(part[step:], 512 - step, 1)
        row_id = lax.broadcasted_iota(jnp.int32, (8, 512), 0)
        for step in (4, 2, 1):
            moved = pltpu.roll(part, 512 - step, 1)
            part = jnp.where((row_id & step) != 0, moved, part)
        far = jnp.sum(acc[side, 3] + acc[side, 4], keepdims=True)
        by_distance = pltpu.roll(jnp.sum(part, axis=0, keepdims=True), SEG_LEN - 1, 1)
        lane = lax.broadcasted_iota(jnp.int32, (1, 512), 1)
        top = TABLE_LEN - 1
        clipped = (lane >= top) & (lane < 448)
        far = far + jnp.sum(jnp.where(clipped, by_distance, 0.0), keepdims=True)
        row = jnp.where(lane < top, by_distance, jnp.where(lane == top, far, 0.0))
        for n in range(4):
            tab[h, n : n + 1, :] = row[:, n * HALF : (n + 1) * HALF]

    def forward(k):
        @pl.when(has_prv)
        def _():
            kv_copy(k, 0).wait_recv()

            @pl.when(has_nxt)
            def _():
                kv_copy(k, 1).start()

        @pl.when(has_nxt)
        def _():
            qg_copy(HEADS - 1 - k, 0).wait_recv()

            @pl.when(has_prv)
            def _():
                qg_copy(HEADS - 1 - k, 1).start()

    def send_own(k):
        @pl.when(has_prv)
        def _():
            send_kv(k)

        @pl.when(has_nxt)
        def _():
            send_qg(k)

    @pl.loop(0, HEADS + 1)
    def _(k):
        in_round(0, k < y_rounds, tell)
        in_round(1, 2 * k < z_rounds, tell)
        in_round(2, k < row_size - 2, tell)

        @pl.when(k < GROUP)
        def _():
            forward(k)

        @pl.when(k < 2)
        def _():
            send_own(k + 2)

        @pl.when(k == GROUP - 1)
        def _():
            pl.loop(GROUP, 6)(send_own)

        in_round(1, 2 * k < z_rounds, hear)
        in_round(1, 2 * k + 1 < z_rounds, tell)

        @pl.when(k >= 1)
        def _():
            ahead, back = k - 1, HEADS - k

            @pl.when(has_prv2)
            def _():
                kv_copy(ahead, 1).wait_recv()

            query_side(ahead)

            @pl.when(k == HEADS - 1)
            def _():
                over_row.start(over_z.total())

            @pl.when(has_nxt2)
            def _():
                qg_copy(back, 1).wait_recv()

            key_side(back)

            @pl.when(k <= GROUP)
            def _():
                table_row(0, ahead)
                table_row(1, back)

        in_round(0, k < y_rounds, hear)
        in_round(2, k < row_size - 2, hear)
        in_round(1, 2 * k + 1 < z_rounds, hear)

        @pl.when(k == GROUP)
        def _():
            for h in range(HEADS):
                half, row = h // GROUP, 3 * (h % GROUP)
                tab_half[half, row : row + 3, :] = tab[h, 0:3, :]
            core_copy.start()
            forward(4)
            core_copy.wait_recv()
            over_y.start(tab_half[at_core] + tab_core[...])
            send_own(6)
            forward(5)
            over_z.start(over_y.total())
            send_own(7)
            pl.loop(6, HEADS)(forward)

    over_row.receive()
    for half in range(2):
        value = tab_row[half * tp_size]
        for x in range(1, tp_size):
            value = value + tab_row[half * tp_size + x]
        for h in range(GROUP):
            for n in range(3):
                width = min(HALF, TABLE_LEN - n * HALF)
                gt_ref[
                    half * GROUP + h : half * GROUP + h + 1, n * HALF : n * HALF + width
                ] = value[3 * h + n : 3 * h + n + 1, :width]

    @pl.when(has_nxt)
    def _():
        @pl.loop(0, HEADS)
        def _(h):
            kv_copy(h, 0).wait_send()

            @pl.when(has_prv)
            def _():
                kv_copy(h, 1).wait_send()

    @pl.when(has_prv)
    def _():
        st_copy(0).wait_send()

        @pl.when(has_nxt)
        def _():
            st_copy(1).wait_send()

        @pl.loop(0, HEADS)
        def _(h):
            qg_copy(h, 0).wait_send()

            @pl.when(has_nxt)
            def _():
                qg_copy(h, 1).wait_send()

    core_copy.wait_send()
    for line in (over_y, over_z, over_row):
        line.finish()


def write_out(*refs):
    count = len(refs) // 2
    copies = [
        pltpu.make_async_copy(refs[n], refs[count + n], refs[-1].at[n]) for n in range(count)
    ]
    for copy in copies:
        copy.start()
    for copy in copies:
        copy.wait()


def solution(mesh):
    sp_size, tp_size = mesh.shape["sp"], mesh.shape["tp"]

    def local(query_rows, key_rows, value_rows, out_grad, log_totals, out_dot, bias_table):
        hbm = pl.BlockSpec(memory_space=pltpu.HBM)
        z_size, y_size, core_size = SP_SHAPE
        tiles = (3 * GROUP, HALF)

        def in_hbm(array):
            return pltpu.with_memory_space_constraint(array, pltpu.HBM)

        vmem = pl.BlockSpec(memory_space=pltpu.VMEM)
        rows = jax.ShapeDtypeStruct(query_rows.shape, BF16)
        shapes = (rows, rows, rows, jax.ShapeDtypeStruct(bias_table.shape, F32))
        results = pl.pallas_call(
            functools.partial(kernel, sp_size, tp_size),
            out_shape=shapes,
            in_specs=[hbm] * 7,
            out_specs=(vmem, vmem, vmem, vmem),
            scratch_shapes=[
                pltpu.VMEM((HEADS, 2, 3 * ROWS, HEAD_DIM), BF16),
                pltpu.VMEM((HEADS, 2, 3 * ROWS, HEAD_DIM), BF16),
                pltpu.VMEM((3, 2 * HEADS, ROWS), F32),
                pltpu.VMEM((3, 2 * HEADS, 8, ROWS), F32),
                pltpu.VMEM((HEADS, 5, HALF, HALF), F32),
                pltpu.VMEM((HEADS, TABLE_LEN), F32),
                pltpu.VMEM((HEADS, 512), F32),
                pltpu.VMEM((2, 5, HALF, HALF), F32),
                pltpu.VMEM((HEADS, 4, HALF), F32),
                pltpu.VMEM((2,) + tiles, F32),
                pltpu.VMEM(tiles, F32),
                pltpu.VMEM((y_size,) + tiles, F32),
                pltpu.VMEM((z_size,) + tiles, F32),
                pltpu.VMEM((core_size * tp_size,) + tiles, F32),
                pltpu.SemaphoreType.DMA((4, HEADS)),
                pltpu.SemaphoreType.DMA((3,)),
                pltpu.SemaphoreType.REGULAR((6,)),
                pltpu.SemaphoreType.DMA((2,)),
                pltpu.SemaphoreType.DMA((y_size,)),
                pltpu.SemaphoreType.DMA((y_size,)),
                pltpu.SemaphoreType.DMA((z_size,)),
                pltpu.SemaphoreType.DMA((z_size,)),
                pltpu.SemaphoreType.DMA((core_size * tp_size,)),
                pltpu.SemaphoreType.DMA((core_size * tp_size,)),
                pltpu.SemaphoreType.DMA((2, HEADS)),
                pltpu.SemaphoreType.DMA((2, HEADS)),
                pltpu.SemaphoreType.DMA((2, HEADS)),
                pltpu.SemaphoreType.DMA((2, HEADS)),
                pltpu.SemaphoreType.DMA((2,)),
                pltpu.SemaphoreType.DMA((2,)),
            ],
            compiler_params=pltpu.CompilerParams(
                collective_id=0, has_side_effects=True, vmem_limit_bytes=32 * 2**20
            ),
        )(*map(in_hbm, (query_rows, key_rows, value_rows, out_grad, log_totals.T, out_dot.T, bias_table)))
        return pl.pallas_call(
            write_out,
            out_shape=shapes,
            in_specs=[vmem] * 4,
            out_specs=(hbm,) * 4,
            scratch_shapes=[pltpu.SemaphoreType.DMA((4,))],
        )(*(pltpu.with_memory_space_constraint(part, pltpu.VMEM) for part in results))

    split = P(("sp", "tp"), None)
    return jax.shard_map(
        local,
        mesh=mesh,
        in_specs=(split,) * 6 + (P(),),
        out_specs=(split, split, split, P()),
        check_vma=False,
    )
```
